32 devices in a mesh: row: 8 (over z, y), col: 4 (over x, core).
Axes of the slice: x: 2, y: 2, z: 4, core: 2. Of those that a mesh axis runs over, the one named last changes fastest.
Arguments:
- tokens: bfloat16 [4096, 2048], P('row'), may hold values from -6 to 6
- outer_weight: bfloat16 [2048, 1024], P(None, 'col'), may hold values from -0.125 to 0.125
- inner_weight: bfloat16 [2048, 1024], P(None, 'col'), may hold values from -0.125 to 0.125
- value_weight: bfloat16 [2048, 1024], P(None, 'col'), may hold values from -0.125 to 0.125
- conv_taps: float32 [3, 3, 1024], P(None, None, 'col'), may hold values from -3.5 to 3.5
- feature_weight: float32 [33, 128], replicated, may hold values from -1 to 1
- feature_phase: float32 [128], replicated, may hold values from -3.140625 to 3.140625
- inner_mats: float32 [2, 128, 128], replicated, may hold values from -0.5 to 0.5
- inner_phase: float32 [2, 128], replicated, may hold values from -3.140625 to 3.140625
- frequency: float32 [128], replicated, may hold values from 0.1 to 1.9
- forward_weight: float32 [128, 1024], P(None, 'col'), may hold values from -0.5 to 0.5
- backward_weight: float32 [128, 1024], P(None, 'col'), may hold values from -0.5 to 0.5
- decay_rate: float32 [1024], P('col'), may hold values from 0.2 to 409.6, as said below
- skip_gain: float32 [1024], P('col'), may hold values from -6 to 6
- output_weight: bfloat16 [1024, 2048], replicated, may hold values from -0.1875 to 0.1875
Outputs:
- layer_out: bfloat16 [4096, 2048], P(('row', 'col'))
The draws below stay inside these ranges and needn't reach their ends.
Inputs may be any that keep to these rules, and one draw needn't show every extreme that they name: `decay_rate`: positive rates of the channels' filter windows.
All inputs are finite; a program needn't handle non-finite values.
Results may differ from the reference program's by a relative error of at most 0.014.
Values may be sent and summed in bfloat16 or wider, within the bound.
A program may use at most 64 MiB of HBM per device.

```python
import math
import jax
import jax.numpy as jnp
from jax import lax

D = 2048
C = 1024
UNITS = 128
BANDS = 16
INNER = 2
LENGTH = 4096


def draw_decay_rate(key, part):
    picker, slow_key, fast_key = jax.random.split(key, 3)
    share = 0.5
    fast_mask = jax.random.uniform(picker, (C,), jnp.float32) < share
    slow_rate = jax.random.uniform(slow_key, (C,), jnp.float32, 0.2, 2.0)
    fast_rate = LENGTH / jax.random.uniform(fast_key, (C,), jnp.float32, 10.0, 30.0)
    return jnp.where(fast_mask, fast_rate, slow_rate).astype(jnp.float32)


def block_scale(own_key, shape, shards, least, largest):
    gain = 1.0
    for position, parts in shards:
        heights = jax.random.uniform(jax.random.fold_in(jax.random.fold_in(own_key, 6), position), (parts,), jnp.float32, least / len(shards), largest / len(shards))
        gain = gain * jnp.repeat(jnp.exp(heights), shape[position] // parts).reshape((-1,) + (1,) * (len(shape) - 1 - position))
    return gain


def centred(own_key, shape, width, limit, cuts=(), kind=jnp.bfloat16):
    values = jax.random.normal(own_key, shape, jnp.float32) * width
    if len(cuts) > 0:
        values = block_scale(own_key, shape, cuts, -0.22, 0.18) * values
    return jnp.clip(values, min=-limit, max=limit).astype(kind)


def setup_inputs(seed: int = 0) -> dict:
    arg_keys = jax.random.split(jax.random.key(seed), 16)
    tokens = centred(arg_keys[0], (LENGTH, D), 1.0, 6.0, ((0, 8),))
    outer_weight = centred(arg_keys[1], (D, C), D ** -0.5, 0.125, ((1, 4),))
    inner_weight = centred(arg_keys[2], (D, C), D ** -0.5, 0.125, ((1, 4),))
    value_weight = centred(arg_keys[3], (D, C), D ** -0.5, 0.125, ((1, 4),))
    conv_taps = centred(arg_keys[4], (3, 3, C), 0.577, 3.5, ((2, 4),), jnp.float32)
    feature_weight = centred(arg_keys[5], (2 * BANDS + 1, UNITS), (2 * BANDS + 1) ** -0.5, 1.0, (), jnp.float32)
    feature_phase = jnp.clip(jax.random.uniform(arg_keys[6], (UNITS,), jnp.float32, -3.140625, 3.140625), -3.140625, 3.140625)
    inner_mats = centred(arg_keys[7], (INNER, UNITS, UNITS), UNITS ** -0.5, 0.5, (), jnp.float32)
    inner_phase = jnp.clip(jax.random.uniform(arg_keys[8], (INNER, UNITS), jnp.float32, -3.140625, 3.140625), -3.140625, 3.140625)
    frequency = jnp.clip(1.0 + 0.18 * jax.random.normal(arg_keys[9], (UNITS,), jnp.float32), 0.1, 1.9)
    forward_weight = centred(arg_keys[10], (UNITS, C), UNITS ** -0.5, 0.5, ((1, 4),), jnp.float32)
    backward_weight = centred(arg_keys[11], (UNITS, C), UNITS ** -0.5, 0.5, ((1, 4),), jnp.float32)
    decay_rate = draw_decay_rate(jax.random.fold_in(arg_keys[15], 71), 0)
    skip_gain = centred(arg_keys[13], (C,), 1.0, 6.0, ((0, 4),), jnp.float32)
    output_weight = centred(arg_keys[14], (C, D), C ** -0.5, 0.1875)
    return {"tokens": tokens, "outer_weight": outer_weight, "inner_weight": inner_weight, "value_weight": value_weight, "conv_taps": conv_taps, "feature_weight": feature_weight, "feature_phase": feature_phase, "inner_mats": inner_mats, "inner_phase": inner_phase, "frequency": frequency, "forward_weight": forward_weight, "backward_weight": backward_weight, "decay_rate": decay_rate, "skip_gain": skip_gain, "output_weight": output_weight}


PRECISE = lax.Precision.HIGHEST

def short_conv(projected, tap_rows):
    padded = jnp.pad(projected.astype(jnp.float32), ((1, 1), (0, 0)))
    return padded[:-2] * tap_rows[0] + padded[1:-1] * tap_rows[1] + padded[2:] * tap_rows[2]

def reference(tokens, outer_weight, inner_weight, value_weight, conv_taps, feature_weight, feature_phase, inner_mats, inner_phase, frequency, forward_weight, backward_weight, decay_rate, skip_gain, output_weight):
    outer_proj = jnp.dot(tokens, outer_weight, preferred_element_type=jnp.float32).astype(jnp.bfloat16)
    inner_proj = jnp.dot(tokens, inner_weight, preferred_element_type=jnp.float32).astype(jnp.bfloat16)
    value_proj = jnp.dot(tokens, value_weight, preferred_element_type=jnp.float32).astype(jnp.bfloat16)
    places = jnp.arange(LENGTH, dtype=jnp.int32)
    scaled = places.astype(jnp.float32) / (LENGTH - 1)
    band_ints = 1 + jnp.arange(BANDS, dtype=jnp.int32) * (LENGTH // (4 * BANDS))
    turns = places[:, None] * band_ints[None, :] % LENGTH
    angles = 2.0 * math.pi / LENGTH * turns.astype(jnp.float32)
    features = jnp.concatenate([scaled[:, None], jnp.cos(angles), -jnp.sin(angles)], axis=1)
    hidden = jnp.sin(frequency * (jnp.dot(features, feature_weight, precision=PRECISE) + feature_phase))
    for level_index in range(INNER):
        hidden = jnp.sin(frequency * (jnp.dot(hidden, inner_mats[level_index], precision=PRECISE) + inner_phase[level_index]))
    channel_block = 128
    block_count = C // channel_block

    def split_cols(matrix):
        return matrix.reshape(matrix.shape[0], block_count, channel_block).transpose(1, 0, 2)

    def one_block(pieces):
        outer_part, inner_part, value_part, tap_block, ahead_cols, behind_cols, rates, skips = pieces
        gate_part = short_conv(outer_part, tap_block[:, 0]).astype(jnp.bfloat16)
        signal = (short_conv(inner_part, tap_block[:, 1]) * short_conv(value_part, tap_block[:, 2])).astype(jnp.bfloat16)
        window = jnp.exp(-scaled[:, None] * rates[None, :])
        filter_ahead = jnp.dot(hidden, ahead_cols, precision=PRECISE) * window
        filter_behind = jnp.dot(hidden, behind_cols, precision=PRECISE) * window
        norm_scale = lax.rsqrt(1.0 + lax.optimization_barrier(jnp.sum(jnp.square(filter_ahead), axis=0)) + lax.optimization_barrier(jnp.sum(jnp.square(filter_behind[1:]), axis=0)))
        kernel = jnp.concatenate([filter_ahead, jnp.zeros((1, channel_block), jnp.float32), filter_behind[:0:-1]], axis=0) * norm_scale
        signal_wide = signal.astype(jnp.float32)
        spectrum = jnp.fft.rfft(signal_wide, n=2 * LENGTH, axis=0) * jnp.fft.rfft(kernel, axis=0)
        response = jnp.fft.irfft(spectrum, n=2 * LENGTH, axis=0)[:LENGTH].astype(jnp.bfloat16)
        response = lax.optimization_barrier(response)
        return (gate_part.astype(jnp.float32) * (response.astype(jnp.float32) + skips * signal_wide)).astype(jnp.bfloat16)
    taps_split = conv_taps.reshape(3, 3, block_count, channel_block).transpose(2, 0, 1, 3)
    mixed_blocks = lax.map(one_block, (split_cols(outer_proj), split_cols(inner_proj), split_cols(value_proj), taps_split, split_cols(forward_weight), split_cols(backward_weight), decay_rate.reshape(block_count, channel_block), skip_gain.reshape(block_count, channel_block)))
    mixed_rows = mixed_blocks.transpose(1, 0, 2).reshape(LENGTH, C)
    return jnp.dot(mixed_rows, output_weight, preferred_element_type=jnp.float32).astype(jnp.bfloat16)
```

```python
import functools
import math

import jax
import jax.numpy as jnp
import numpy as np
from jax import lax
from jax.experimental import pallas as pl
from jax.experimental.pallas import tpu as pltpu
from jax.sharding import PartitionSpec as P

BANDS = 16
INNER = 2
FACTOR = 256


PRECISE = lax.Precision.HIGHEST


def with_halo(array, sides, width):
    for axis, dim in sides:
        devices, length = (lax.axis_size(axis), array.shape[dim])
        up = [(i, (i + 1) % devices) for i in range(devices - 1)]
        down = [(j, i) for i, j in up]
        last = lax.slice_in_dim(array, length - width, length, axis=dim)
        leading = lax.slice_in_dim(array, 0, width, axis=dim)
        before = lax.ppermute(last, axis, up)
        after = lax.ppermute(leading, axis, down)
        array = jnp.concatenate([before, array, after], axis=dim)
    return array


def phases(height, breadth, period):
    row_index = lax.broadcasted_iota(jnp.int32, (height, breadth), 0)
    col_index = lax.broadcasted_iota(jnp.int32, (height, breadth), 1)
    phase_angle = 2.0 * math.pi / period * (row_index * col_index % period).astype(jnp.float32)
    return (jnp.cos(phase_angle), jnp.sin(phase_angle))


def along_last(operand, matrix):
    return jnp.einsum("ckb,bj->ckj", operand, matrix, precision=PRECISE)


def forward_transform(operand, tables):
    cosine_one, sine_one, twist_cos, twist_sin, cosine_two, sine_two = tables
    used_rows = operand.shape[1]
    first_real = jnp.einsum("kr,crb->ckb", cosine_one[:, :used_rows], operand, precision=PRECISE)
    first_imag = -jnp.einsum("kr,crb->ckb", sine_one[:, :used_rows], operand, precision=PRECISE)
    turned_real = first_real * twist_cos + first_imag * twist_sin
    turned_imag = first_imag * twist_cos - first_real * twist_sin
    spec_real = along_last(turned_real, cosine_two) + along_last(turned_imag, sine_two)
    spec_imag = along_last(turned_imag, cosine_two) - along_last(turned_real, sine_two)
    return (spec_real, spec_imag)


def inverse_transform(spec_real, spec_imag, tables, kept_rows):
    cosine_one, sine_one, twist_cos, twist_sin, cosine_two, sine_two = tables
    back_real = along_last(spec_real, cosine_two) - along_last(spec_imag, sine_two)
    back_imag = along_last(spec_imag, cosine_two) + along_last(spec_real, sine_two)
    untwist_real = back_real * twist_cos - back_imag * twist_sin
    untwist_imag = back_imag * twist_cos + back_real * twist_sin
    return jnp.einsum(
        "nk,ckb->cnb", cosine_one[:kept_rows], untwist_real, precision=PRECISE
    ) - jnp.einsum("nk,ckb->cnb", sine_one[:kept_rows], untwist_imag, precision=PRECISE)


def position_filters(
    places,
    seq_length,
    feature_weight,
    feature_phase,
    inner_mats,
    inner_phase,
    frequency,
    forward_cols,
    backward_cols,
    rates,
):
    scaled = places.astype(jnp.float32) / (seq_length - 1)
    band_ints = 1 + jnp.arange(BANDS, dtype=jnp.int32) * (seq_length // (4 * BANDS))
    turns = places[:, None] * band_ints[None, :] % seq_length
    angles = 2.0 * math.pi / seq_length * turns.astype(jnp.float32)
    features = jnp.concatenate([scaled[:, None], jnp.cos(angles), -jnp.sin(angles)], axis=1)
    hidden = jnp.sin(
        frequency * (jnp.dot(features, feature_weight, precision=PRECISE) + feature_phase)
    )
    for level_index in range(INNER):
        hidden = jnp.sin(
            frequency
            * (
                jnp.dot(hidden, inner_mats[level_index], precision=PRECISE)
                + inner_phase[level_index]
            )
        )
    window = jnp.exp(-scaled[:, None] * rates[None, :])
    filter_ahead = jnp.dot(hidden, forward_cols, precision=PRECISE) * window
    filter_behind = jnp.dot(hidden, backward_cols, precision=PRECISE) * window
    return (filter_ahead, filter_behind)


def on_device(
    tokens,
    outer_weight,
    inner_weight,
    value_weight,
    conv_taps,
    feature_weight,
    feature_phase,
    inner_mats,
    inner_phase,
    frequency,
    forward_weight,
    backward_weight,
    decay_rate,
    skip_gain,
    output_weight,
):
    block_rows = tokens.shape[0]
    seq_length = block_rows * lax.axis_size("row")
    own_width = outer_weight.shape[1]
    outer_proj = jnp.dot(tokens, outer_weight, preferred_element_type=jnp.float32).astype(
        jnp.bfloat16
    )
    inner_proj = jnp.dot(tokens, inner_weight, preferred_element_type=jnp.float32).astype(
        jnp.bfloat16
    )
    value_proj = jnp.dot(tokens, value_weight, preferred_element_type=jnp.float32).astype(
        jnp.bfloat16
    )
    stacked = jnp.concatenate([outer_proj, inner_proj, value_proj], axis=1)
    padded = with_halo(stacked, (("row", 0),), 1).astype(jnp.float32)
    tap_table = conv_taps.reshape(3, 3 * own_width)
    convolved = padded[:-2] * tap_table[0] + padded[1:-1] * tap_table[1] + padded[2:] * tap_table[2]
    gate_part = convolved[:, :own_width].astype(jnp.bfloat16)
    signal = (convolved[:, own_width : 2 * own_width] * convolved[:, 2 * own_width :]).astype(
        jnp.bfloat16
    )
    offset = lax.axis_index("row") * block_rows
    places = offset + jnp.arange(block_rows, dtype=jnp.int32)
    filter_ahead, filter_behind = position_filters(
        places,
        seq_length,
        feature_weight,
        feature_phase,
        inner_mats,
        inner_phase,
        frequency,
        forward_weight,
        backward_weight,
        decay_rate,
    )
    moved_signal, moved_ahead, moved_behind = (
        lax.all_to_all(signal.astype(jnp.float32), "row", split_axis=1, concat_axis=0, tiled=True),
        lax.all_to_all(filter_ahead, "row", split_axis=1, concat_axis=0, tiled=True),
        lax.all_to_all(filter_behind, "row", split_axis=1, concat_axis=0, tiled=True),
    )
    per_device = moved_ahead.shape[1]
    ahead_rows = moved_ahead.T
    behind_rows = moved_behind.T
    norm_scale = lax.rsqrt(
        1.0
        + jnp.sum(jnp.square(ahead_rows), axis=1)
        + jnp.sum(jnp.square(behind_rows[:, 1:]), axis=1)
    )
    kernel_rows = (
        jnp.concatenate(
            [ahead_rows, jnp.zeros((per_device, 1), jnp.float32), jnp.flip(behind_rows[:, 1:], 1)],
            axis=1,
        )
        * norm_scale[:, None]
    )
    padded_length = 2 * seq_length
    height = padded_length // FACTOR
    tables = (
        phases(height, height, height)
        + phases(height, FACTOR, padded_length)
        + phases(FACTOR, FACTOR, FACTOR)
    )
    kernel_real, kernel_imag = forward_transform(
        kernel_rows.reshape(per_device, height, FACTOR), tables
    )
    signal_real, signal_imag = forward_transform(
        moved_signal.T.reshape(per_device, height // 2, FACTOR), tables
    )
    prod_real = signal_real * kernel_real - signal_imag * kernel_imag
    prod_imag = signal_real * kernel_imag + signal_imag * kernel_real
    response = inverse_transform(prod_real, prod_imag, tables, height // 2) / padded_length
    response = response.reshape(per_device, seq_length).T.astype(jnp.bfloat16)
    returned = lax.all_to_all(response, "row", split_axis=0, concat_axis=1, tiled=True)
    mixed_rows = (
        gate_part.astype(jnp.float32)
        * (returned.astype(jnp.float32) + skip_gain * signal.astype(jnp.float32))
    ).astype(jnp.bfloat16)
    whole_rows = lax.all_to_all(mixed_rows, "col", split_axis=0, concat_axis=1, tiled=True)
    return jnp.dot(whole_rows, output_weight, preferred_element_type=jnp.float32).astype(
        jnp.bfloat16
    )


WIDE = 256


def feature_table(seq_length):
    places = np.arange(seq_length, dtype=np.int64)
    bands = 1 + np.arange(BANDS, dtype=np.int64) * (seq_length // (4 * BANDS))
    angles = 2.0 * np.pi / seq_length * (places[:, None] * bands[None, :] % seq_length)
    scaled = places / (seq_length - 1)
    feats = np.concatenate([scaled[:, None], np.cos(angles), -np.sin(angles)], 1).astype(np.float32)
    high = feats.astype(jnp.bfloat16)
    low = (feats - high.astype(np.float32)).astype(jnp.bfloat16)
    ones = np.ones((seq_length, 2), jnp.bfloat16)
    used = np.concatenate([high, low, high, ones], 1)
    return np.pad(used, ((0, 0), (0, 128 - used.shape[1])))


def sine_coefficients():
    u = 0.5 * np.cos(np.pi * (np.arange(4000) + 0.5) / 8000)
    powers = np.stack([u ** (2 * i + 1) for i in range(6)], 1)
    return [float(v) for v in np.linalg.lstsq(powers, np.sin(2 * np.pi * u), rcond=None)[0]]


SINE = sine_coefficients()
MAGIC = 12582912.0


def sine_of_turns(turns):
    u = turns - ((turns + MAGIC) - MAGIC)
    square = u * u
    total = SINE[-1]
    for value in SINE[-2::-1]:
        total = total * square + value
    return u * total


def split_two(value):
    high = value.astype(jnp.bfloat16)
    return high, (value - high.astype(jnp.float32)).astype(jnp.bfloat16)


def combine(terms):
    total = None
    for coef, array in terms:
        if abs(coef) < 1e-9:
            continue
        if abs(abs(coef) - 1.0) < 1e-9:
            if total is None:
                total = array if coef > 0 else -array
            else:
                total = total + array if coef > 0 else total - array
        else:
            total = array * coef if total is None else total + array * coef
    return total


def first_stage(planes):
    half = len(planes)
    full, mid = 2 * half, half // 2
    quarter = mid // 2
    theta = 2 * math.pi / full
    add = {r: planes[r] + planes[half - r] for r in range(1, mid)}
    sub = {r: planes[r] - planes[half - r] for r in range(1, mid)}
    add_add = {r: add[r] + add[mid - r] for r in range(1, quarter)}
    add_sub = {r: add[r] - add[mid - r] for r in range(1, quarter)}
    sub_add = {r: sub[r] + sub[mid - r] for r in range(1, quarter)}
    sub_sub = {r: sub[r] - sub[mid - r] for r in range(1, quarter)}
    ends = (planes[0] + planes[mid], planes[0] - planes[mid])
    out = []
    for k in range(half + 1):
        cos = lambda r: math.cos(theta * r * k)
        sin = lambda r: math.sin(theta * r * k)
        if k % 4 == 0:
            real = combine([(1.0, ends[0]), (cos(quarter), add[quarter])] + [(cos(r), add_add[r]) for r in add_add])
            imag = combine([(-sin(r), sub_sub[r]) for r in sub_sub])
        elif k % 2 == 0:
            real = combine([(1.0, ends[1])] + [(cos(r), add_sub[r]) for r in add_sub])
            imag = combine([(-sin(quarter), sub[quarter])] + [(-sin(r), sub_add[r]) for r in sub_add])
        else:
            real = combine([(1.0, planes[0])] + [(cos(r), sub[r]) for r in sub])
            imag = combine([(-sin(mid), planes[mid])] + [(-sin(r), add[r]) for r in add])
        out.append((real, imag))
    return out


def last_stage(pairs):
    half = len(pairs) - 1
    full, mid = 2 * half, half // 2
    quarter = mid // 2
    theta = 2 * math.pi / full
    four = range(0, half + 1, 4)
    two = range(2, half + 1, 4)
    odd = range(1, half + 1, 2)
    real = [p[0] for p in pairs]
    imag = [p[1] for p in pairs]
    out = [None] * half

    def cosines(r, ks):
        return combine([(math.cos(theta * r * k), real[k]) for k in ks])

    def sines(r, ks):
        return combine([(math.sin(theta * r * k), imag[k]) for k in ks])

    out[0] = combine([(1.0, v) for v in real])
    out[mid] = cosines(mid, list(four) + list(two)) - sines(mid, odd)

    def place(r, cos_even, sin_even):
        cos_odd, sin_odd = cosines(r, odd), sines(r, odd)
        out[r] = (cos_even - sin_even) + (cos_odd - sin_odd)
        out[half - r] = (cos_even + sin_even) - (cos_odd + sin_odd)

    for r in range(1, quarter):
        c0, c2, s0, s2 = cosines(r, four), cosines(r, two), sines(r, four), sines(r, two)
        place(r, c0 + c2, s0 + s2)
        place(mid - r, c0 - c2, s2 - s0)
    place(quarter, cosines(quarter, four), sines(quarter, two))
    return out


def front_kernel(tokens, edges, outer, inner, value, taps, gate_ref, signal_ref, moved_ref, acc, edge_acc):
    step = pl.program_id(0)
    width = outer.shape[1]

    @pl.when(step == 0)
    def _():
        acc[...] = jnp.zeros_like(acc)
        edge_acc[...] = jnp.zeros_like(edge_acc)

    for j, weight in enumerate((outer, inner, value)):
        cols = slice(j * width, (j + 1) * width)
        acc[:, cols] += jnp.dot(tokens[...], weight[...], preferred_element_type=jnp.float32)
        edge_acc[:, cols] += jnp.dot(edges[...], weight[...], preferred_element_type=jnp.float32)

    @pl.when(step == pl.num_programs(0) - 1)
    def _():
        rows = acc.shape[0]
        parts = []
        index = lax.broadcasted_iota(jnp.int32, (rows, width), 0)
        for j in range(3):
            cols = slice(j * width, (j + 1) * width)
            proj = acc[:, cols].astype(jnp.bfloat16).astype(jnp.float32)
            ends = edge_acc[:, cols].astype(jnp.bfloat16).astype(jnp.float32)
            before = jnp.where(index == 0, ends[0:1], pltpu.roll(proj, 1, 0))
            after = jnp.where(index == rows - 1, ends[1:2], pltpu.roll(proj, rows - 1, 0))
            parts.append(before * taps[j : j + 1, :] + proj * taps[3 + j : 4 + j, :] + after * taps[6 + j : 7 + j, :])
        gate_ref[...] = parts[0].astype(jnp.bfloat16)
        signal = (parts[1] * parts[2]).astype(jnp.bfloat16)
        signal_ref[...] = signal
        groups, members, _ = moved_ref.shape
        flipped = signal.astype(jnp.float32).T.astype(jnp.bfloat16)
        for g in range(groups):
            moved_ref[g] = flipped[g * members : (g + 1) * members]


def spectrum_kernel(feats, first_w, inner_w, inner_p, both_w, rates, twist_c, twist_s, cos_t, sin_t,
                    real_ref, imag_ref, sums, diffs, turned):
    length = feats.shape[0]
    count = rates.shape[0]
    chunk = min(512, length)

    def one_chunk(i, carry):
        at = pl.ds(pl.multiple_of(i * chunk, chunk), chunk)
        hidden = sine_of_turns(jnp.dot(feats[at, :], first_w[...], preferred_element_type=jnp.float32))
        for level in range(INNER):
            high, low = split_two(hidden)
            wide = jnp.dot(jnp.concatenate([high, low], 1), inner_w[level], preferred_element_type=jnp.float32)
            hidden = sine_of_turns(wide[:, :128] + wide[:, 128:] + inner_p[level : level + 1, :])
        both = lax.dot_general(both_w[...], hidden.astype(jnp.bfloat16), (((1,), (1,)), ((), ())),
                               preferred_element_type=jnp.float32)
        place = lax.broadcasted_iota(jnp.int32, (count, chunk), 1) + i * chunk
        window = jnp.exp(place.astype(jnp.float32) * (-1.0 / (length - 1)) * rates[...])
        ahead = both[:count] * window
        behind = jnp.where(place == 0, 0.0, both[count:] * window)
        sums[:, at] = ahead + behind
        diffs[:, at] = ahead - behind
        return carry + jnp.sum(ahead * ahead + behind * behind, axis=1, keepdims=True)

    energy = lax.fori_loop(0, length // chunk, one_chunk, jnp.zeros((count, 1), jnp.float32))
    scale = lax.rsqrt(1.0 + energy) * (0.5 / length)
    planes = length // WIDE
    for top in range(0, count, 16):
        for left in range(0, WIDE, 128):
            for which, source in enumerate((sums, diffs)):
                got = [source[top : top + 16, r * WIDE + left : r * WIDE + left + 128] * scale[top : top + 16] for r in range(planes)]
                for k, (real, imag) in enumerate(first_stage(got)):
                    weight = 1.0 if k in (0, planes) else 2.0
                    c = twist_c[k : k + 1, left : left + 128] * weight
                    s = twist_s[k : k + 1, left : left + 128] * weight
                    rows = slice(k * count + top, k * count + top + 16)
                    cols = slice(left, left + 128)
                    if imag is None:
                        new_real, new_imag = real * c, -(real * s)
                    else:
                        new_real, new_imag = real * c + imag * s, imag * c - real * s
                    turned[2 * which, rows, cols] = new_real.astype(jnp.bfloat16)
                    turned[2 * which + 1, rows, cols] = new_imag.astype(jnp.bfloat16)
    dot = functools.partial(jnp.dot, preferred_element_type=jnp.float32)
    real_ref[...] = dot(turned[0], cos_t[...]) + dot(turned[1], sin_t[...])
    imag_ref[...] = dot(turned[3], cos_t[...]) - dot(turned[2], sin_t[...])


def convolve_kernel(moved, filt_real, filt_imag, twist_c, twist_s, cos_t, sin_t, out_ref, turned, back):
    senders, count, block = moved.shape
    per = block // WIDE
    planes = senders * per
    dot = functools.partial(jnp.dot, preferred_element_type=jnp.float32)
    for top in range(0, count, 16):
        for left in range(0, WIDE, 128):
            got = [moved[r // per, top : top + 16, (r % per) * WIDE + left : (r % per) * WIDE + left + 128].astype(jnp.float32) for r in range(planes)]
            for k, (real, imag) in enumerate(first_stage(got)):
                c, s = twist_c[k : k + 1, left : left + 128], twist_s[k : k + 1, left : left + 128]
                rows = slice(k * count + top, k * count + top + 16)
                cols = slice(left, left + 128)
                if imag is None:
                    new_real, new_imag = real * c, -(real * s)
                else:
                    new_real, new_imag = real * c + imag * s, imag * c - real * s
                turned[0, rows, cols] = new_real.astype(jnp.bfloat16)
                turned[1, rows, cols] = new_imag.astype(jnp.bfloat16)
    real = dot(turned[0], cos_t[...]) + dot(turned[1], sin_t[...])
    imag = dot(turned[1], cos_t[...]) - dot(turned[0], sin_t[...])
    prod_real = (real * filt_real[...] - imag * filt_imag[...]).astype(jnp.bfloat16)
    prod_imag = (real * filt_imag[...] + imag * filt_real[...]).astype(jnp.bfloat16)
    back[0] = dot(prod_real, cos_t[...]) - dot(prod_imag, sin_t[...])
    back[1] = dot(prod_imag, cos_t[...]) + dot(prod_real, sin_t[...])
    for top in range(0, count, 16):
        for left in range(0, WIDE, 128):
            cols = slice(left, left + 128)
            pairs = []
            for k in range(planes + 1):
                c, s = twist_c[k : k + 1, cols], twist_s[k : k + 1, cols]
                rows = slice(k * count + top, k * count + top + 16)
                b_real, b_imag = back[0, rows, cols], back[1, rows, cols]
                pairs.append((b_real * c - b_imag * s, b_imag * c + b_real * s))
            for r, plane in enumerate(last_stage(pairs)):
                at = (r % per) * WIDE + left
                out_ref[r // per, top : top + 16, at : at + 128] = plane.astype(jnp.bfloat16)


def mix_kernel(response, gate, signal, skip, out_ref):
    groups, members, block = response.shape
    flipped = jnp.concatenate([response[g].astype(jnp.float32) for g in range(groups)], 0).T
    mixed = gate[...].astype(jnp.float32) * (flipped + skip[...] * signal[...].astype(jnp.float32))
    out_ref[...] = mixed.astype(jnp.bfloat16)


def whole(count):
    return [pl.BlockSpec(memory_space=pltpu.VMEM)] * count


def fits(tokens_rows, seq_length, own_width, row_devices, units):
    planes = seq_length // WIDE
    members = own_width // row_devices
    return (
        own_width % 128 == 0
        and members % 16 == 0
        and tokens_rows % WIDE == 0
        and seq_length % 512 == 0
        and planes % 8 == 0
        and 8 <= planes <= 32
        and units == 128
    )


def on_device_fast(
    tokens, outer_weight, inner_weight, value_weight, conv_taps, feature_weight, feature_phase,
    inner_mats, inner_phase, frequency, forward_weight, backward_weight, decay_rate, skip_gain, output_weight,
):
    f32, bf16 = jnp.float32, jnp.bfloat16
    rows, depth = tokens.shape
    devices = lax.axis_size("row")
    seq_length = rows * devices
    width = outer_weight.shape[1]
    members = width // devices
    planes = seq_length // WIDE
    up = [(i, i + 1) for i in range(devices - 1)]
    down = [(j, i) for i, j in up]
    before = lax.ppermute(tokens[-1:], "row", up)
    after = lax.ppermute(tokens[:1], "row", down)
    edges = jnp.concatenate([before, after, jnp.zeros((14, depth), bf16)], 0)

    me = lax.axis_index("row")
    turn = frequency / (2.0 * math.pi)
    first = feature_weight * turn
    first_high, first_low = split_two(first)
    phase_high, phase_low = split_two(feature_phase * turn)
    first_w = jnp.concatenate([first_high, first_high, first_low, phase_high[None], phase_low[None]], 0)
    first_w = jnp.pad(first_w, ((0, 128 - first_w.shape[0]), (0, 0)))
    mats_high, mats_low = split_two(inner_mats * turn)
    inner_w = jnp.concatenate(
        [jnp.concatenate([mats_high, mats_low], 2), jnp.concatenate([mats_high, jnp.zeros_like(mats_low)], 2)], 1
    )
    own = functools.partial(lax.dynamic_slice_in_dim, start_index=me * members, slice_size=members)
    both_w = jnp.concatenate([own(forward_weight, axis=1).T, own(backward_weight, axis=1).T], 0).astype(bf16)
    rates = own(decay_rate, axis=0)[:, None]
    k_index = np.arange(planes + 1)[:, None] * np.arange(WIDE)[None, :]
    twist_c = jnp.asarray(np.cos(2 * np.pi * k_index / (2 * seq_length)), f32)
    twist_s = jnp.asarray(np.sin(2 * np.pi * k_index / (2 * seq_length)), f32)
    w_index = np.arange(WIDE)[:, None] * np.arange(WIDE)[None, :] % WIDE
    cos_t = jnp.asarray(np.cos(2 * np.pi * w_index / WIDE), bf16)
    sin_t = jnp.asarray(np.sin(2 * np.pi * w_index / WIDE), bf16)
    tables = (twist_c, twist_s, cos_t, sin_t)
    spec_rows = (planes + 1) * members
    spec = jax.ShapeDtypeStruct((spec_rows, WIDE), f32)
    filt_real, filt_imag = pl.pallas_call(
        spectrum_kernel,
        out_shape=(spec, spec),
        in_specs=whole(10),
        out_specs=tuple(whole(2)),
        scratch_shapes=[
            pltpu.VMEM((members, seq_length), f32),
            pltpu.VMEM((members, seq_length), f32),
            pltpu.VMEM((4, spec_rows, WIDE), bf16),
        ],
        cost_estimate=pl.CostEstimate(flops=3 * 10**9, bytes_accessed=4 * 10**6, transcendentals=0),
        name="spectrum",
    )(jnp.asarray(feature_table(seq_length)), first_w, inner_w, inner_phase * turn, both_w, rates, *tables)

    step = 512 if depth % 512 == 0 else depth
    weight_spec = pl.BlockSpec((step, width), lambda k: (k, 0))
    fixed = lambda *shape: pl.BlockSpec(shape, lambda k: (0,) * len(shape))
    gate, signal, moved = pl.pallas_call(
        front_kernel,
        grid=(depth // step,),
        in_specs=[
            pl.BlockSpec((rows, step), lambda k: (0, k)),
            pl.BlockSpec((16, step), lambda k: (0, k)),
            weight_spec, weight_spec, weight_spec,
            fixed(9, width),
        ],
        out_specs=(fixed(rows, width), fixed(rows, width), fixed(devices, members, rows)),
        out_shape=(
            jax.ShapeDtypeStruct((rows, width), bf16),
            jax.ShapeDtypeStruct((rows, width), bf16),
            jax.ShapeDtypeStruct((devices, members, rows), bf16),
        ),
        scratch_shapes=[pltpu.VMEM((rows, 3 * width), f32), pltpu.VMEM((16, 3 * width), f32)],
        cost_estimate=pl.CostEstimate(flops=2 * rows * depth * 3 * width, bytes_accessed=6 * 10**6, transcendentals=0),
        name="front",
    )(tokens, edges, outer_weight, inner_weight, value_weight, conv_taps.reshape(9, width))
    moved = lax.all_to_all(moved, "row", split_axis=0, concat_axis=0)
    response = pl.pallas_call(
        convolve_kernel,
        out_shape=jax.ShapeDtypeStruct((devices, members, rows), bf16),
        in_specs=whole(7),
        out_specs=whole(1)[0],
        scratch_shapes=[pltpu.VMEM((2, spec_rows, WIDE), bf16), pltpu.VMEM((2, spec_rows, WIDE), f32)],
        cost_estimate=pl.CostEstimate(flops=2 * 10**9, bytes_accessed=2 * 10**6, transcendentals=0),
        name="convolve",
    )(moved, filt_real, filt_imag, *tables)
    response = lax.all_to_all(response, "row", split_axis=0, concat_axis=0)
    mixed = pl.pallas_call(
        mix_kernel,
        out_shape=jax.ShapeDtypeStruct((rows, width), bf16),
        in_specs=whole(4),
        out_specs=whole(1)[0],
        name="mix",
    )(response, gate, signal, skip_gain[None, :])
    parts = lax.axis_size("col")
    spread = lax.all_to_all(mixed.reshape(parts, rows // parts, width), "col", split_axis=0, concat_axis=0)
    whole_rows = spread.transpose(1, 0, 2).reshape(rows // parts, parts * width)
    return jnp.dot(whole_rows, output_weight, preferred_element_type=f32).astype(bf16)


def on_any(*args):
    tokens, outer_weight, feature_weight = args[0], args[1], args[5]
    devices = lax.axis_size("row")
    if fits(tokens.shape[0], tokens.shape[0] * devices, outer_weight.shape[1], devices, feature_weight.shape[1]):
        return on_device_fast(*args)
    return on_device(*args)


def solution(mesh):
    placed = (
        P("row", None),
        P(None, "col"),
        P(None, "col"),
        P(None, "col"),
        P(None, None, "col"),
        P(),
        P(),
        P(),
        P(),
        P(),
        P(None, "col"),
        P(None, "col"),
        P("col"),
        P("col"),
        P(),
    )
    return jax.shard_map(
        on_any, mesh=mesh, in_specs=placed, out_specs=P(("row", "col"), None), check_vma=False
    )
```

```python
import functools
import math

import jax
import jax.numpy as jnp
import numpy as np
from jax import lax
from jax.experimental import pallas as pl
from jax.experimental.pallas import tpu as pltpu
from jax.sharding import PartitionSpec as P

BANDS = 16
INNER = 2
FACTOR = 256


PRECISE = lax.Precision.HIGHEST


def with_halo(array, sides, width):
    for axis, dim in sides:
        devices, length = (lax.axis_size(axis), array.shape[dim])
        up = [(i, (i + 1) % devices) for i in range(devices - 1)]
        down = [(j, i) for i, j in up]
        last = lax.slice_in_dim(array, length - width, length, axis=dim)
        leading = lax.slice_in_dim(array, 0, width, axis=dim)
        before = lax.ppermute(last, axis, up)
        after = lax.ppermute(leading, axis, down)
        array = jnp.concatenate([before, array, after], axis=dim)
    return array


def phases(height, breadth, period):
    row_index = lax.broadcasted_iota(jnp.int32, (height, breadth), 0)
    col_index = lax.broadcasted_iota(jnp.int32, (height, breadth), 1)
    phase_angle = 2.0 * math.pi / period * (row_index * col_index % period).astype(jnp.float32)
    return (jnp.cos(phase_angle), jnp.sin(phase_angle))


def along_last(operand, matrix):
    return jnp.einsum("ckb,bj->ckj", operand, matrix, precision=PRECISE)


def forward_transform(operand, tables):
    cosine_one, sine_one, twist_cos, twist_sin, cosine_two, sine_two = tables
    used_rows = operand.shape[1]
    first_real = jnp.einsum("kr,crb->ckb", cosine_one[:, :used_rows], operand, precision=PRECISE)
    first_imag = -jnp.einsum("kr,crb->ckb", sine_one[:, :used_rows], operand, precision=PRECISE)
    turned_real = first_real * twist_cos + first_imag * twist_sin
    turned_imag = first_imag * twist_cos - first_real * twist_sin
    spec_real = along_last(turned_real, cosine_two) + along_last(turned_imag, sine_two)
    spec_imag = along_last(turned_imag, cosine_two) - along_last(turned_real, sine_two)
    return (spec_real, spec_imag)


def inverse_transform(spec_real, spec_imag, tables, kept_rows):
    cosine_one, sine_one, twist_cos, twist_sin, cosine_two, sine_two = tables
    back_real = along_last(spec_real, cosine_two) - along_last(spec_imag, sine_two)
    back_imag = along_last(spec_imag, cosine_two) + along_last(spec_real, sine_two)
    untwist_real = back_real * twist_cos - back_imag * twist_sin
    untwist_imag = back_imag * twist_cos + back_real * twist_sin
    return jnp.einsum(
        "nk,ckb->cnb", cosine_one[:kept_rows], untwist_real, precision=PRECISE
    ) - jnp.einsum("nk,ckb->cnb", sine_one[:kept_rows], untwist_imag, precision=PRECISE)


def position_filters(
    places,
    seq_length,
    feature_weight,
    feature_phase,
    inner_mats,
    inner_phase,
    frequency,
    forward_cols,
    backward_cols,
    rates,
):
    scaled = places.astype(jnp.float32) / (seq_length - 1)
    band_ints = 1 + jnp.arange(BANDS, dtype=jnp.int32) * (seq_length // (4 * BANDS))
    turns = places[:, None] * band_ints[None, :] % seq_length
    angles = 2.0 * math.pi / seq_length * turns.astype(jnp.float32)
    features = jnp.concatenate([scaled[:, None], jnp.cos(angles), -jnp.sin(angles)], axis=1)
    hidden = jnp.sin(
        frequency * (jnp.dot(features, feature_weight, precision=PRECISE) + feature_phase)
    )
    for level_index in range(INNER):
        hidden = jnp.sin(
            frequency
            * (
                jnp.dot(hidden, inner_mats[level_index], precision=PRECISE)
                + inner_phase[level_index]
            )
        )
    window = jnp.exp(-scaled[:, None] * rates[None, :])
    filter_ahead = jnp.dot(hidden, forward_cols, precision=PRECISE) * window
    filter_behind = jnp.dot(hidden, backward_cols, precision=PRECISE) * window
    return (filter_ahead, filter_behind)


def on_device(
    tokens,
    outer_weight,
    inner_weight,
    value_weight,
    conv_taps,
    feature_weight,
    feature_phase,
    inner_mats,
    inner_phase,
    frequency,
    forward_weight,
    backward_weight,
    decay_rate,
    skip_gain,
    output_weight,
):
    block_rows = tokens.shape[0]
    seq_length = block_rows * lax.axis_size("row")
    own_width = outer_weight.shape[1]
    outer_proj = jnp.dot(tokens, outer_weight, preferred_element_type=jnp.float32).astype(
        jnp.bfloat16
    )
    inner_proj = jnp.dot(tokens, inner_weight, preferred_element_type=jnp.float32).astype(
        jnp.bfloat16
    )
    value_proj = jnp.dot(tokens, value_weight, preferred_element_type=jnp.float32).astype(
        jnp.bfloat16
    )
    stacked = jnp.concatenate([outer_proj, inner_proj, value_proj], axis=1)
    padded = with_halo(stacked, (("row", 0),), 1).astype(jnp.float32)
    tap_table = conv_taps.reshape(3, 3 * own_width)
    convolved = padded[:-2] * tap_table[0] + padded[1:-1] * tap_table[1] + padded[2:] * tap_table[2]
    gate_part = convolved[:, :own_width].astype(jnp.bfloat16)
    signal = (convolved[:, own_width : 2 * own_width] * convolved[:, 2 * own_width :]).astype(
        jnp.bfloat16
    )
    offset = lax.axis_index("row") * block_rows
    places = offset + jnp.arange(block_rows, dtype=jnp.int32)
    filter_ahead, filter_behind = position_filters(
        places,
        seq_length,
        feature_weight,
        feature_phase,
        inner_mats,
        inner_phase,
        frequency,
        forward_weight,
        backward_weight,
        decay_rate,
    )
    moved_signal, moved_ahead, moved_behind = (
        lax.all_to_all(signal.astype(jnp.float32), "row", split_axis=1, concat_axis=0, tiled=True),
        lax.all_to_all(filter_ahead, "row", split_axis=1, concat_axis=0, tiled=True),
        lax.all_to_all(filter_behind, "row", split_axis=1, concat_axis=0, tiled=True),
    )
    per_device = moved_ahead.shape[1]
    ahead_rows = moved_ahead.T
    behind_rows = moved_behind.T
    norm_scale = lax.rsqrt(
        1.0
        + jnp.sum(jnp.square(ahead_rows), axis=1)
        + jnp.sum(jnp.square(behind_rows[:, 1:]), axis=1)
    )
    kernel_rows = (
        jnp.concatenate(
            [ahead_rows, jnp.zeros((per_device, 1), jnp.float32), jnp.flip(behind_rows[:, 1:], 1)],
            axis=1,
        )
        * norm_scale[:, None]
    )
    padded_length = 2 * seq_length
    height = padded_length // FACTOR
    tables = (
        phases(height, height, height)
        + phases(height, FACTOR, padded_length)
        + phases(FACTOR, FACTOR, FACTOR)
    )
    kernel_real, kernel_imag = forward_transform(
        kernel_rows.reshape(per_device, height, FACTOR), tables
    )
    signal_real, signal_imag = forward_transform(
        moved_signal.T.reshape(per_device, height // 2, FACTOR), tables
    )
    prod_real = signal_real * kernel_real - signal_imag * kernel_imag
    prod_imag = signal_real * kernel_imag + signal_imag * kernel_real
    response = inverse_transform(prod_real, prod_imag, tables, height // 2) / padded_length
    response = response.reshape(per_device, seq_length).T.astype(jnp.bfloat16)
    returned = lax.all_to_all(response, "row", split_axis=0, concat_axis=1, tiled=True)
    mixed_rows = (
        gate_part.astype(jnp.float32)
        * (returned.astype(jnp.float32) + skip_gain * signal.astype(jnp.float32))
    ).astype(jnp.bfloat16)
    whole_rows = lax.all_to_all(mixed_rows, "col", split_axis=0, concat_axis=1, tiled=True)
    return jnp.dot(whole_rows, output_weight, preferred_element_type=jnp.float32).astype(
        jnp.bfloat16
    )


WIDE = 256


def feature_table(seq_length):
    places = np.arange(seq_length, dtype=np.int64)
    bands = 1 + np.arange(BANDS, dtype=np.int64) * (seq_length // (4 * BANDS))
    angles = 2.0 * np.pi / seq_length * (places[:, None] * bands[None, :] % seq_length)
    scaled = places / (seq_length - 1)
    feats = np.concatenate([scaled[:, None], np.cos(angles), -np.sin(angles)], 1).astype(np.float32)
    high = feats.astype(jnp.bfloat16)
    low = (feats - high.astype(np.float32)).astype(jnp.bfloat16)
    used = np.zeros((seq_length, 128), jnp.bfloat16)
    count = feats.shape[1]
    for start, part in ((0, high), (40, low), (80, high)):
        used[:, start : start + count] = part
    used[:, 120:122] = 1
    return used


def sine_coefficients():
    u = 0.5 * np.cos(np.pi * (np.arange(4000) + 0.5) / 8000)
    powers = np.stack([u ** (2 * i + 1) for i in range(6)], 1)
    return [float(v) for v in np.linalg.lstsq(powers, np.sin(2 * np.pi * u), rcond=None)[0]]


SINE = sine_coefficients()
MAGIC = 12582912.0


def sine_of_turns(turns):
    u = turns - ((turns + MAGIC) - MAGIC)
    square = u * u
    total = SINE[-1]
    for value in SINE[-2::-1]:
        total = total * square + value
    return u * total


def split_two(value):
    high = value.astype(jnp.bfloat16)
    return high, (value - high.astype(jnp.float32)).astype(jnp.bfloat16)


def combine(terms):
    total = None
    for coef, array in terms:
        if abs(coef) < 1e-9:
            continue
        if abs(abs(coef) - 1.0) < 1e-9:
            if total is None:
                total = array if coef > 0 else -array
            else:
                total = total + array if coef > 0 else total - array
        else:
            total = array * coef if total is None else total + array * coef
    return total


def first_stage(planes):
    half = len(planes)
    full, mid = 2 * half, half // 2
    quarter = mid // 2
    theta = 2 * math.pi / full
    add = {r: planes[r] + planes[half - r] for r in range(1, mid)}
    sub = {r: planes[r] - planes[half - r] for r in range(1, mid)}
    add_add = {r: add[r] + add[mid - r] for r in range(1, quarter)}
    add_sub = {r: add[r] - add[mid - r] for r in range(1, quarter)}
    sub_add = {r: sub[r] + sub[mid - r] for r in range(1, quarter)}
    sub_sub = {r: sub[r] - sub[mid - r] for r in range(1, quarter)}
    ends = (planes[0] + planes[mid], planes[0] - planes[mid])
    out = []
    for k in range(half + 1):
        cos = lambda r: math.cos(theta * r * k)
        sin = lambda r: math.sin(theta * r * k)
        if k % 4 == 0:
            real = combine([(1.0, ends[0]), (cos(quarter), add[quarter])] + [(cos(r), add_add[r]) for r in add_add])
            imag = combine([(-sin(r), sub_sub[r]) for r in sub_sub])
        elif k % 2 == 0:
            real = combine([(1.0, ends[1])] + [(cos(r), add_sub[r]) for r in add_sub])
            imag = combine([(-sin(quarter), sub[quarter])] + [(-sin(r), sub_add[r]) for r in sub_add])
        else:
            real = combine([(1.0, planes[0])] + [(cos(r), sub[r]) for r in sub])
            imag = combine([(-sin(mid), planes[mid])] + [(-sin(r), add[r]) for r in add])
        out.append((real, imag))
    return out


def last_stage(pairs):
    half = len(pairs) - 1
    full, mid = 2 * half, half // 2
    quarter = mid // 2
    theta = 2 * math.pi / full
    four = range(0, half + 1, 4)
    two = range(2, half + 1, 4)
    odd = range(1, half + 1, 2)
    real = [p[0] for p in pairs]
    imag = [p[1] for p in pairs]
    out = [None] * half

    def cosines(r, ks):
        return combine([(math.cos(theta * r * k), real[k]) for k in ks])

    def sines(r, ks):
        return combine([(math.sin(theta * r * k), imag[k]) for k in ks])

    out[0] = combine([(1.0, v) for v in real])
    out[mid] = cosines(mid, list(four) + list(two)) - sines(mid, odd)

    def place(r, cos_even, sin_even):
        cos_odd, sin_odd = cosines(r, odd), sines(r, odd)
        out[r] = (cos_even - sin_even) + (cos_odd - sin_odd)
        out[half - r] = (cos_even + sin_even) - (cos_odd + sin_odd)

    for r in range(1, quarter):
        c0, c2, s0, s2 = cosines(r, four), cosines(r, two), sines(r, four), sines(r, two)
        place(r, c0 + c2, s0 + s2)
        place(mid - r, c0 - c2, s2 - s0)
    place(quarter, cosines(quarter, four), sines(quarter, two))
    return out


def tiles(count, body):
    lanes = WIDE // 128

    def one(i, carry):
        body(pl.multiple_of(i // lanes * 16, 16), pl.multiple_of(i % lanes * 128, 128))
        return carry

    lax.fori_loop(0, count // 16 * lanes, one, 0)


def layer_kernel(
    tokens_h, outer_h, inner_h, value_h, out_weight_h, feats_h,
    taps, feature_weight, feature_phase, inner_mats, inner_phase, frequency, forward, backward, rate, skip,
    twist_c, twist_s, cos_t, sin_t,
    out_ref,
    tok, weights, out_weight, feats, sig_send, sig_recv, resp_send, resp_recv, mix_send, mix_recv,
    sums, diffs, turned, filt, back, scale_ref, first_ref, chan, rate_col, energy_ref, gate_ref, signal_ref,
    local_sem, edge_send, edge_recv, sig_s, sig_r, resp_s, resp_r, mix_s, mix_r,
):
    f32, bf16 = jnp.float32, jnp.bfloat16
    dot = functools.partial(jnp.dot, preferred_element_type=f32)
    n_row, n_col = lax.axis_size("row"), lax.axis_size("col")
    row, col = lax.axis_index("row"), lax.axis_index("col")
    length, rows = feats.shape[0], tokens_h.shape[0]
    width = outer_h.shape[1]
    count = width // n_row
    planes = length // WIDE
    per = rows // WIDE
    mesh_id = pl.DeviceIdType.MESH

    barrier = pltpu.get_barrier_semaphore()
    for o in range(1, n_row):
        pl.semaphore_signal(barrier, inc=1, device_id=(lax.rem(row + o, n_row), col), device_id_type=mesh_id)
    for o in range(1, n_col):
        pl.semaphore_signal(barrier, inc=1, device_id=(row, lax.rem(col + o, n_col)), device_id_type=mesh_id)
    loads = [
        pltpu.make_async_copy(feats_h, feats, local_sem.at[0]),
        pltpu.make_async_copy(tokens_h, tok.at[pl.ds(0, rows)], local_sem.at[1]),
        pltpu.make_async_copy(inner_h, weights.at[1], local_sem.at[2]),
        pltpu.make_async_copy(value_h, weights.at[2], local_sem.at[3]),
        pltpu.make_async_copy(outer_h, weights.at[0], local_sem.at[4]),
        pltpu.make_async_copy(out_weight_h, out_weight, local_sem.at[5]),
    ]
    for load in loads:
        load.start()

    turn = frequency[...] * (0.5 / math.pi)
    high, low = split_two(feature_weight[...] * turn)
    phase_high, phase_low = split_two(feature_phase[...] * turn)
    used = high.shape[0]
    first_ref[...] = jnp.zeros_like(first_ref)
    first_ref[0:used] = high.astype(f32)
    first_ref[40 : 40 + used] = high.astype(f32)
    first_ref[80 : 80 + used] = low.astype(f32)
    first_ref[120:121] = phase_high.astype(f32)
    first_ref[121:122] = phase_low.astype(f32)
    first_w = first_ref[...].astype(bf16)
    inner_w = []
    for level in range(INNER):
        mat_high, mat_low = split_two(inner_mats[level] * turn)
        inner_w.append(jnp.concatenate([
            jnp.concatenate([mat_high, mat_low], 1), jnp.concatenate([mat_high, jnp.zeros_like(mat_low)], 1)], 0))
    inner_p = inner_phase[...] * turn
    chan[0] = forward[...].T
    chan[1] = backward[...].T
    rate_col[...] = jnp.broadcast_to(rate[...], (128, width)).T
    own = pl.ds(pl.multiple_of(row * count, 16), count)
    both_w = jnp.concatenate([chan[0, own, :], chan[1, own, :]], 0).astype(bf16)
    rates = rate_col[own, 0:1]
    chunk = 512
    energy_ref[...] = jnp.zeros_like(energy_ref)

    def one_chunk(i, carry):
        at = pl.ds(pl.multiple_of(i * chunk, chunk), chunk)
        hidden = sine_of_turns(dot(feats[at, :], first_w))
        for level in range(INNER):
            h_high, h_low = split_two(hidden)
            wide = dot(jnp.concatenate([h_high, h_low], 1), inner_w[level])
            hidden = sine_of_turns(wide[:, :128] + wide[:, 128:] + inner_p[level : level + 1, :])
        both = lax.dot_general(both_w, hidden.astype(bf16), (((1,), (1,)), ((), ())), preferred_element_type=f32)
        place = lax.broadcasted_iota(jnp.int32, (count, chunk), 1) + i * chunk
        window = jnp.exp(place.astype(f32) * (-1.0 / (length - 1)) * rates)
        ahead = both[:count] * window
        behind = jnp.where(place == 0, 0.0, both[count:] * window)
        sums[:, at] = ahead + behind
        diffs[:, at] = ahead - behind
        energy_ref[...] += jnp.broadcast_to(
            jnp.sum(ahead * ahead + behind * behind, axis=1, keepdims=True), (count, 128))
        return carry

    early = min(EARLY, length // chunk)
    loads[0].wait()
    lax.fori_loop(0, early, one_chunk, 0)

    pl.semaphore_wait(barrier, n_row + n_col - 2)
    edges = [
        pltpu.make_async_remote_copy(
            src_ref=tokens_h.at[pl.ds(rows - 16 if i == 0 else 0, 16)],
            dst_ref=tok.at[pl.ds(rows + 16 * i, 16)],
            send_sem=edge_send.at[i], recv_sem=edge_recv.at[i],
            device_id=(lax.rem(row + (1 if i == 0 else n_row - 1), n_row), col), device_id_type=mesh_id)
        for i in range(2)
    ]
    for edge in edges:
        edge.start()
    loads[1].wait()
    loads[2].wait()
    loads[3].wait()
    for edge in edges:
        edge.wait()

    index = lax.broadcasted_iota(jnp.int32, (rows, width), 0)
    has_before = jnp.where(row > 0, 1.0, 0.0)
    has_after = jnp.where(row < n_row - 1, 1.0, 0.0)

    def convolved(j):
        proj = dot(tok[...], weights[j]).astype(bf16).astype(f32)
        main = proj[:rows]
        first = proj[rows + 15 : rows + 16] * has_before
        last = proj[rows + 16 : rows + 17] * has_after
        before = jnp.where(index == 0, first, pltpu.roll(main, 1, 0))
        after = jnp.where(index == rows - 1, last, pltpu.roll(main, rows - 1, 0))
        return before * taps[0, j : j + 1, :] + main * taps[1, j : j + 1, :] + after * taps[2, j : j + 1, :]

    signal = (convolved(1) * convolved(2)).astype(bf16)
    signal_ref[...] = signal
    flipped = signal.astype(f32).T.astype(bf16)
    for g in range(n_row):
        sig_send[g] = flipped[g * count : (g + 1) * count]

    def exchange(send, recv, s_sem, r_sem, size, me, target):
        copies = []
        for o in range(1, size):
            peer = lax.rem(me + o, size)
            copies.append(pltpu.make_async_remote_copy(
                src_ref=send.at[peer], dst_ref=recv.at[me],
                send_sem=s_sem.at[o], recv_sem=r_sem.at[o], device_id=target(peer), device_id_type=mesh_id))
        for copy in copies:
            copy.start()
        recv[me] = send[me]
        return copies

    along_row = lambda peer: (peer, col)
    along_col = lambda peer: (row, peer)
    travelling = exchange(sig_send, sig_recv, sig_s, sig_r, n_row, row, along_row)

    loads[4].wait()
    gate_ref[...] = convolved(0).astype(bf16)
    lax.fori_loop(early, length // chunk, one_chunk, 0)
    scale_ref[...] = lax.rsqrt(1.0 + energy_ref[...]) * (0.5 / length)

    def turn_into(first, pairs, top, left, weighted):
        for k, (real, imag) in enumerate(pairs):
            c, s = twist_c[k : k + 1, pl.ds(left, 128)], twist_s[k : k + 1, pl.ds(left, 128)]
            if weighted and k not in (0, planes):
                c, s = c * 2.0, s * 2.0
            at = pl.ds(pl.multiple_of(k * count + top, 16), 16)
            if imag is None:
                new_real, new_imag = real * c, -(real * s)
            else:
                new_real, new_imag = real * c + imag * s, imag * c - real * s
            turned[first, at, pl.ds(left, 128)] = new_real.astype(bf16)
            turned[first + 1, at, pl.ds(left, 128)] = new_imag.astype(bf16)

    def filter_tile(top, left):
        scale = scale_ref[pl.ds(top, 16), :]
        for which, source in enumerate((sums, diffs)):
            got = [source[pl.ds(top, 16), pl.ds(pl.multiple_of(r * WIDE + left, 128), 128)] * scale for r in range(planes)]
            turn_into(2 * which, first_stage(got), top, left, True)

    tiles(count, filter_tile)
    filt[0] = dot(turned[0], cos_t[...]) + dot(turned[1], sin_t[...])
    filt[1] = dot(turned[3], cos_t[...]) - dot(turned[2], sin_t[...])
    for copy in travelling:
        copy.wait()

    def signal_tile(top, left):
        got = [sig_recv[r // per, pl.ds(top, 16), pl.ds(pl.multiple_of(r % per * WIDE + left, 128), 128)].astype(f32)
               for r in range(planes)]
        turn_into(0, first_stage(got), top, left, False)

    tiles(count, signal_tile)
    real = dot(turned[0], cos_t[...]) + dot(turned[1], sin_t[...])
    imag = dot(turned[1], cos_t[...]) - dot(turned[0], sin_t[...])
    prod_real = (real * filt[0] - imag * filt[1]).astype(bf16)
    prod_imag = (real * filt[1] + imag * filt[0]).astype(bf16)
    back[0] = dot(prod_real, cos_t[...]) - dot(prod_imag, sin_t[...])
    back[1] = dot(prod_imag, cos_t[...]) + dot(prod_real, sin_t[...])

    def back_tile(top, left):
        pairs = []
        for k in range(planes + 1):
            c, s = twist_c[k : k + 1, pl.ds(left, 128)], twist_s[k : k + 1, pl.ds(left, 128)]
            at = pl.ds(pl.multiple_of(k * count + top, 16), 16)
            b_real, b_imag = back[0, at, pl.ds(left, 128)], back[1, at, pl.ds(left, 128)]
            pairs.append((b_real * c - b_imag * s, b_imag * c + b_real * s))
        for r, plane in enumerate(last_stage(pairs)):
            at = pl.multiple_of(r % per * WIDE + left, 128)
            resp_send[r // per, pl.ds(top, 16), pl.ds(at, 128)] = plane.astype(bf16)

    tiles(count, back_tile)
    for copy in exchange(resp_send, resp_recv, resp_s, resp_r, n_row, row, along_row):
        copy.wait()
    response = jnp.concatenate([resp_recv[g].astype(f32) for g in range(n_row)], 0).T
    mixed = (gate_ref[...].astype(f32) * (response + skip[...] * signal_ref[...].astype(f32))).astype(bf16)
    share = rows // n_col
    for p in range(n_col):
        mix_send[p] = mixed[p * share : (p + 1) * share]
    travelling = exchange(mix_send, mix_recv, mix_s, mix_r, n_col, col, along_col)
    loads[5].wait()
    for copy in travelling:
        copy.wait()
    left_side = jnp.concatenate([mix_recv[p] for p in range(n_col)], 1)
    out_width = out_ref.shape[1]
    for j in range(0, out_width, 512):
        out_ref[:, j : j + 512] = dot(left_side, out_weight[:, j : j + 512]).astype(bf16)


EARLY = 2


def fits(tokens_rows, seq_length, own_width, row_devices, units):
    planes = seq_length // WIDE
    members = own_width // row_devices
    return (
        own_width % 128 == 0
        and members % 16 == 0
        and tokens_rows % WIDE == 0
        and seq_length % 512 == 0
        and planes % 8 == 0
        and 8 <= planes <= 32
        and units == 128
        and tokens_rows % 64 == 0
    )


def on_device_fast(
    tokens, outer_weight, inner_weight, value_weight, conv_taps, feature_weight, feature_phase,
    inner_mats, inner_phase, frequency, forward_weight, backward_weight, decay_rate, skip_gain, output_weight,
):
    f32, bf16 = jnp.float32, jnp.bfloat16
    rows, depth = tokens.shape
    devices = lax.axis_size("row")
    seq_length = rows * devices
    width = outer_weight.shape[1]
    members = width // devices
    planes = seq_length // WIDE
    n_col = lax.axis_size("col")
    k_index = np.arange(planes + 1)[:, None] * np.arange(WIDE)[None, :]
    twist_c = jnp.asarray(np.cos(2 * np.pi * k_index / (2 * seq_length)), f32)
    twist_s = jnp.asarray(np.sin(2 * np.pi * k_index / (2 * seq_length)), f32)
    w_index = np.arange(WIDE)[:, None] * np.arange(WIDE)[None, :] % WIDE
    cos_t = jnp.asarray(np.cos(2 * np.pi * w_index / WIDE), bf16)
    sin_t = jnp.asarray(np.sin(2 * np.pi * w_index / WIDE), bf16)
    spec_rows = (planes + 1) * members
    any_spec = pl.BlockSpec(memory_space=pl.ANY)
    vmem = pl.BlockSpec(memory_space=pltpu.VMEM)
    dma = pltpu.SemaphoreType.DMA
    share = rows // n_col
    out_width = output_weight.shape[1]
    exchanged = pltpu.VMEM((devices, members, rows), bf16)
    spread = pltpu.VMEM((n_col, share, width), bf16)
    return pl.pallas_call(
        layer_kernel,
        out_shape=jax.ShapeDtypeStruct((share, out_width), bf16),
        in_specs=[any_spec] * 6 + [vmem] * 14,
        out_specs=vmem,
        scratch_shapes=[
            pltpu.VMEM((rows + 32, depth), bf16),
            pltpu.VMEM((3, depth, width), bf16),
            pltpu.VMEM(output_weight.shape, bf16),
            pltpu.VMEM((seq_length, 128), bf16),
            exchanged, exchanged, exchanged, exchanged, spread, spread,
            pltpu.VMEM((members, seq_length), f32),
            pltpu.VMEM((members, seq_length), f32),
            pltpu.VMEM((4, spec_rows, WIDE), bf16),
            pltpu.VMEM((2, spec_rows, WIDE), f32),
            pltpu.VMEM((2, spec_rows, WIDE), f32),
            pltpu.VMEM((members, 128), f32),
            pltpu.VMEM((128, 128), f32),
            pltpu.VMEM((2, width, 128), f32),
            pltpu.VMEM((width, 128), f32),
            pltpu.VMEM((members, 128), f32),
            pltpu.VMEM((rows, width), bf16),
            pltpu.VMEM((rows, width), bf16),
            dma((6,)), dma((2,)), dma((2,)),
            dma((devices,)), dma((devices,)), dma((devices,)), dma((devices,)), dma((n_col,)), dma((n_col,)),
        ],
        compiler_params=pltpu.CompilerParams(
            collective_id=0, has_side_effects=True, vmem_limit_bytes=56 * 1024 * 1024),
        name="layer",
    )(
        tokens, outer_weight, inner_weight, value_weight, output_weight, jnp.asarray(feature_table(seq_length)),
        conv_taps, feature_weight, feature_phase[None], inner_mats, inner_phase, frequency[None],
        forward_weight, backward_weight, decay_rate[None], skip_gain[None], twist_c, twist_s, cos_t, sin_t,
    )


def on_any(*args):
    tokens, outer_weight, feature_weight = args[0], args[1], args[5]
    devices = lax.axis_size("row")
    if fits(tokens.shape[0], tokens.shape[0] * devices, outer_weight.shape[1], devices, feature_weight.shape[1]):
        return on_device_fast(*args)
    return on_device(*args)


def solution(mesh):
    placed = (
        P("row", None),
        P(None, "col"),
        P(None, "col"),
        P(None, "col"),
        P(None, None, "col"),
        P(),
        P(),
        P(),
        P(),
        P(),
        P(None, "col"),
        P(None, "col"),
        P("col"),
        P("col"),
        P(),
    )
    return jax.shard_map(
        on_any, mesh=mesh, in_specs=placed, out_specs=P(("row", "col"), None), check_vma=False
    )
```

```python
import functools
import math

import jax
import jax.numpy as jnp
import numpy as np
from jax import lax
from jax.experimental import pallas as pl
from jax.experimental.pallas import tpu as pltpu
from jax.sharding import PartitionSpec as P

BANDS = 16
INNER = 2
FACTOR = 256


PRECISE = lax.Precision.HIGHEST


def with_halo(array, sides, width):
    for axis, dim in sides:
        devices, length = (lax.axis_size(axis), array.shape[dim])
        up = [(i, (i + 1) % devices) for i in range(devices - 1)]
        down = [(j, i) for i, j in up]
        last = lax.slice_in_dim(array, length - width, length, axis=dim)
        leading = lax.slice_in_dim(array, 0, width, axis=dim)
        before = lax.ppermute(last, axis, up)
        after = lax.ppermute(leading, axis, down)
        array = jnp.concatenate([before, array, after], axis=dim)
    return array


def phases(height, breadth, period):
    row_index = lax.broadcasted_iota(jnp.int32, (height, breadth), 0)
    col_index = lax.broadcasted_iota(jnp.int32, (height, breadth), 1)
    phase_angle = 2.0 * math.pi / period * (row_index * col_index % period).astype(jnp.float32)
    return (jnp.cos(phase_angle), jnp.sin(phase_angle))


def along_last(operand, matrix):
    return jnp.einsum("ckb,bj->ckj", operand, matrix, precision=PRECISE)


def forward_transform(operand, tables):
    cosine_one, sine_one, twist_cos, twist_sin, cosine_two, sine_two = tables
    used_rows = operand.shape[1]
    first_real = jnp.einsum("kr,crb->ckb", cosine_one[:, :used_rows], operand, precision=PRECISE)
    first_imag = -jnp.einsum("kr,crb->ckb", sine_one[:, :used_rows], operand, precision=PRECISE)
    turned_real = first_real * twist_cos + first_imag * twist_sin
    turned_imag = first_imag * twist_cos - first_real * twist_sin
    spec_real = along_last(turned_real, cosine_two) + along_last(turned_imag, sine_two)
    spec_imag = along_last(turned_imag, cosine_two) - along_last(turned_real, sine_two)
    return (spec_real, spec_imag)


def inverse_transform(spec_real, spec_imag, tables, kept_rows):
    cosine_one, sine_one, twist_cos, twist_sin, cosine_two, sine_two = tables
    back_real = along_last(spec_real, cosine_two) - along_last(spec_imag, sine_two)
    back_imag = along_last(spec_imag, cosine_two) + along_last(spec_real, sine_two)
    untwist_real = back_real * twist_cos - back_imag * twist_sin
    untwist_imag = back_imag * twist_cos + back_real * twist_sin
    return jnp.einsum(
        "nk,ckb->cnb", cosine_one[:kept_rows], untwist_real, precision=PRECISE
    ) - jnp.einsum("nk,ckb->cnb", sine_one[:kept_rows], untwist_imag, precision=PRECISE)


def position_filters(
    places,
    seq_length,
    feature_weight,
    feature_phase,
    inner_mats,
    inner_phase,
    frequency,
    forward_cols,
    backward_cols,
    rates,
):
    scaled = places.astype(jnp.float32) / (seq_length - 1)
    band_ints = 1 + jnp.arange(BANDS, dtype=jnp.int32) * (seq_length // (4 * BANDS))
    turns = places[:, None] * band_ints[None, :] % seq_length
    angles = 2.0 * math.pi / seq_length * turns.astype(jnp.float32)
    features = jnp.concatenate([scaled[:, None], jnp.cos(angles), -jnp.sin(angles)], axis=1)
    hidden = jnp.sin(
        frequency * (jnp.dot(features, feature_weight, precision=PRECISE) + feature_phase)
    )
    for level_index in range(INNER):
        hidden = jnp.sin(
            frequency
            * (
                jnp.dot(hidden, inner_mats[level_index], precision=PRECISE)
                + inner_phase[level_index]
            )
        )
    window = jnp.exp(-scaled[:, None] * rates[None, :])
    filter_ahead = jnp.dot(hidden, forward_cols, precision=PRECISE) * window
    filter_behind = jnp.dot(hidden, backward_cols, precision=PRECISE) * window
    return (filter_ahead, filter_behind)


def on_device(
    tokens,
    outer_weight,
    inner_weight,
    value_weight,
    conv_taps,
    feature_weight,
    feature_phase,
    inner_mats,
    inner_phase,
    frequency,
    forward_weight,
    backward_weight,
    decay_rate,
    skip_gain,
    output_weight,
):
    block_rows = tokens.shape[0]
    seq_length = block_rows * lax.axis_size("row")
    own_width = outer_weight.shape[1]
    outer_proj = jnp.dot(tokens, outer_weight, preferred_element_type=jnp.float32).astype(
        jnp.bfloat16
    )
    inner_proj = jnp.dot(tokens, inner_weight, preferred_element_type=jnp.float32).astype(
        jnp.bfloat16
    )
    value_proj = jnp.dot(tokens, value_weight, preferred_element_type=jnp.float32).astype(
        jnp.bfloat16
    )
    stacked = jnp.concatenate([outer_proj, inner_proj, value_proj], axis=1)
    padded = with_halo(stacked, (("row", 0),), 1).astype(jnp.float32)
    tap_table = conv_taps.reshape(3, 3 * own_width)
    convolved = padded[:-2] * tap_table[0] + padded[1:-1] * tap_table[1] + padded[2:] * tap_table[2]
    gate_part = convolved[:, :own_width].astype(jnp.bfloat16)
    signal = (convolved[:, own_width : 2 * own_width] * convolved[:, 2 * own_width :]).astype(
        jnp.bfloat16
    )
    offset = lax.axis_index("row") * block_rows
    places = offset + jnp.arange(block_rows, dtype=jnp.int32)
    filter_ahead, filter_behind = position_filters(
        places,
        seq_length,
        feature_weight,
        feature_phase,
        inner_mats,
        inner_phase,
        frequency,
        forward_weight,
        backward_weight,
        decay_rate,
    )
    moved_signal, moved_ahead, moved_behind = (
        lax.all_to_all(signal.astype(jnp.float32), "row", split_axis=1, concat_axis=0, tiled=True),
        lax.all_to_all(filter_ahead, "row", split_axis=1, concat_axis=0, tiled=True),
        lax.all_to_all(filter_behind, "row", split_axis=1, concat_axis=0, tiled=True),
    )
    per_device = moved_ahead.shape[1]
    ahead_rows = moved_ahead.T
    behind_rows = moved_behind.T
    norm_scale = lax.rsqrt(
        1.0
        + jnp.sum(jnp.square(ahead_rows), axis=1)
        + jnp.sum(jnp.square(behind_rows[:, 1:]), axis=1)
    )
    kernel_rows = (
        jnp.concatenate(
            [ahead_rows, jnp.zeros((per_device, 1), jnp.float32), jnp.flip(behind_rows[:, 1:], 1)],
            axis=1,
        )
        * norm_scale[:, None]
    )
    padded_length = 2 * seq_length
    height = padded_length // FACTOR
    tables = (
        phases(height, height, height)
        + phases(height, FACTOR, padded_length)
        + phases(FACTOR, FACTOR, FACTOR)
    )
    kernel_real, kernel_imag = forward_transform(
        kernel_rows.reshape(per_device, height, FACTOR), tables
    )
    signal_real, signal_imag = forward_transform(
        moved_signal.T.reshape(per_device, height // 2, FACTOR), tables
    )
    prod_real = signal_real * kernel_real - signal_imag * kernel_imag
    prod_imag = signal_real * kernel_imag + signal_imag * kernel_real
    response = inverse_transform(prod_real, prod_imag, tables, height // 2) / padded_length
    response = response.reshape(per_device, seq_length).T.astype(jnp.bfloat16)
    returned = lax.all_to_all(response, "row", split_axis=0, concat_axis=1, tiled=True)
    mixed_rows = (
        gate_part.astype(jnp.float32)
        * (returned.astype(jnp.float32) + skip_gain * signal.astype(jnp.float32))
    ).astype(jnp.bfloat16)
    whole_rows = lax.all_to_all(mixed_rows, "col", split_axis=0, concat_axis=1, tiled=True)
    return jnp.dot(whole_rows, output_weight, preferred_element_type=jnp.float32).astype(
        jnp.bfloat16
    )


WIDE = 256


def feature_table(seq_length):
    places = np.arange(seq_length, dtype=np.int64)
    bands = 1 + np.arange(BANDS, dtype=np.int64) * (seq_length // (4 * BANDS))
    angles = 2.0 * np.pi / seq_length * (places[:, None] * bands[None, :] % seq_length)
    scaled = places / (seq_length - 1)
    feats = np.concatenate([scaled[:, None], np.cos(angles), -np.sin(angles)], 1).astype(np.float32)
    high = feats.astype(jnp.bfloat16)
    low = (feats - high.astype(np.float32)).astype(jnp.bfloat16)
    used = np.zeros((seq_length, 128), jnp.bfloat16)
    count = feats.shape[1]
    for start, part in ((0, high), (40, low), (80, high)):
        used[:, start : start + count] = part
    used[:, 120:122] = 1
    return used


def sine_coefficients():
    u = 0.5 * np.cos(np.pi * (np.arange(4000) + 0.5) / 8000)
    powers = np.stack([u ** (2 * i + 1) for i in range(6)], 1)
    return [float(v) for v in np.linalg.lstsq(powers, np.sin(2 * np.pi * u), rcond=None)[0]]


SINE = sine_coefficients()
MAGIC = 12582912.0


def sine_of_turns(turns):
    u = turns - ((turns + MAGIC) - MAGIC)
    square = u * u
    total = SINE[-1]
    for value in SINE[-2::-1]:
        total = total * square + value
    return u * total


def split_two(value):
    high = value.astype(jnp.bfloat16)
    return high, (value - high.astype(jnp.float32)).astype(jnp.bfloat16)


def combine(terms):
    total = None
    for coef, array in terms:
        if abs(coef) < 1e-9:
            continue
        if abs(abs(coef) - 1.0) < 1e-9:
            if total is None:
                total = array if coef > 0 else -array
            else:
                total = total + array if coef > 0 else total - array
        else:
            total = array * coef if total is None else total + array * coef
    return total


def first_stage(planes):
    half = len(planes)
    full, mid = 2 * half, half // 2
    quarter = mid // 2
    theta = 2 * math.pi / full
    add = {r: planes[r] + planes[half - r] for r in range(1, mid)}
    sub = {r: planes[r] - planes[half - r] for r in range(1, mid)}
    add_add = {r: add[r] + add[mid - r] for r in range(1, quarter)}
    add_sub = {r: add[r] - add[mid - r] for r in range(1, quarter)}
    sub_add = {r: sub[r] + sub[mid - r] for r in range(1, quarter)}
    sub_sub = {r: sub[r] - sub[mid - r] for r in range(1, quarter)}
    ends = (planes[0] + planes[mid], planes[0] - planes[mid])
    out = []
    for k in range(half + 1):
        cos = lambda r: math.cos(theta * r * k)
        sin = lambda r: math.sin(theta * r * k)
        if k % 4 == 0:
            real = combine([(1.0, ends[0]), (cos(quarter), add[quarter])] + [(cos(r), add_add[r]) for r in add_add])
            imag = combine([(-sin(r), sub_sub[r]) for r in sub_sub])
        elif k % 2 == 0:
            real = combine([(1.0, ends[1])] + [(cos(r), add_sub[r]) for r in add_sub])
            imag = combine([(-sin(quarter), sub[quarter])] + [(-sin(r), sub_add[r]) for r in sub_add])
        else:
            real = combine([(1.0, planes[0])] + [(cos(r), sub[r]) for r in sub])
            imag = combine([(-sin(mid), planes[mid])] + [(-sin(r), add[r]) for r in add])
        out.append((real, imag))
    return out


def last_stage(pairs):
    half = len(pairs) - 1
    full, mid = 2 * half, half // 2
    quarter = mid // 2
    theta = 2 * math.pi / full
    four = range(0, half + 1, 4)
    two = range(2, half + 1, 4)
    odd = range(1, half + 1, 2)
    real = [p[0] for p in pairs]
    imag = [p[1] for p in pairs]
    out = [None] * half

    def cosines(r, ks):
        return combine([(math.cos(theta * r * k), real[k]) for k in ks])

    def sines(r, ks):
        return combine([(math.sin(theta * r * k), imag[k]) for k in ks])

    out[0] = combine([(1.0, v) for v in real])
    out[mid] = cosines(mid, list(four) + list(two)) - sines(mid, odd)

    def place(r, cos_even, sin_even):
        cos_odd, sin_odd = cosines(r, odd), sines(r, odd)
        out[r] = (cos_even - sin_even) + (cos_odd - sin_odd)
        out[half - r] = (cos_even + sin_even) - (cos_odd + sin_odd)

    for r in range(1, quarter):
        c0, c2, s0, s2 = cosines(r, four), cosines(r, two), sines(r, four), sines(r, two)
        place(r, c0 + c2, s0 + s2)
        place(mid - r, c0 - c2, s2 - s0)
    place(quarter, cosines(quarter, four), sines(quarter, two))
    return out


def tiles(count, body):
    lanes = WIDE // 128

    def one(i, carry):
        body(pl.multiple_of(i // lanes * 16, 16), pl.multiple_of(i % lanes * 128, 128))
        return carry

    lax.fori_loop(0, count // 16 * lanes, one, 0)


def layer_kernel(
    tokens_h, outer_h, inner_h, value_h, feats_h,
    taps, feature_weight, feature_phase, inner_mats, inner_phase, frequency, forward, backward, rate, skip,
    twist_c, twist_s, cos_t, sin_t,
    out_ref,
    tok, weights, feats, hid, sig_send, sig_recv, resp_send, resp_recv, mix_send, mix_recv,
    sums, diffs, turned, filt, back, scale_ref, first_ref, chan, rate_col, energy_ref, gate_ref, signal_ref,
    local_sem, edge_send, edge_recv, hid_s, hid_r, sig_s, sig_r, resp_s, resp_r, mix_s, mix_r,
):
    f32, bf16 = jnp.float32, jnp.bfloat16
    dot = functools.partial(jnp.dot, preferred_element_type=f32)
    n_row, n_col = lax.axis_size("row"), lax.axis_size("col")
    row, col = lax.axis_index("row"), lax.axis_index("col")
    length, rows = feats_h.shape[0], tokens_h.shape[0]
    quarter = length // n_col
    width = outer_h.shape[1]
    count = width // n_row
    planes = length // WIDE
    per = rows // WIDE
    mesh_id = pl.DeviceIdType.MESH

    barrier = pltpu.get_barrier_semaphore()
    for o in range(1, n_row):
        pl.semaphore_signal(barrier, inc=1, device_id=(lax.rem(row + o, n_row), col), device_id_type=mesh_id)
    for o in range(1, n_col):
        pl.semaphore_signal(barrier, inc=1, device_id=(row, lax.rem(col + o, n_col)), device_id_type=mesh_id)
    loads = [
        pltpu.make_async_copy(
            feats_h.at[pl.ds(pl.multiple_of(col * quarter, 512), quarter)], feats, local_sem.at[0]),
        pltpu.make_async_copy(tokens_h, tok.at[pl.ds(0, rows)], local_sem.at[1]),
        pltpu.make_async_copy(inner_h, weights.at[1], local_sem.at[2]),
        pltpu.make_async_copy(value_h, weights.at[2], local_sem.at[3]),
        pltpu.make_async_copy(outer_h, weights.at[0], local_sem.at[4]),
    ]
    for load in loads:
        load.start()

    turn = frequency[...] * (0.5 / math.pi)
    high, low = split_two(feature_weight[...] * turn)
    phase_high, phase_low = split_two(feature_phase[...] * turn)
    used = high.shape[0]
    first_ref[...] = jnp.zeros_like(first_ref)
    first_ref[0:used] = high.astype(f32)
    first_ref[40 : 40 + used] = high.astype(f32)
    first_ref[80 : 80 + used] = low.astype(f32)
    first_ref[120:121] = phase_high.astype(f32)
    first_ref[121:122] = phase_low.astype(f32)
    first_w = first_ref[...].astype(bf16)
    inner_w = []
    for level in range(INNER):
        mat_high, mat_low = split_two(inner_mats[level] * turn)
        inner_w.append(jnp.concatenate([
            jnp.concatenate([mat_high, mat_low], 1), jnp.concatenate([mat_high, jnp.zeros_like(mat_low)], 1)], 0))
    inner_p = inner_phase[...] * turn
    chan[0] = forward[...].T
    chan[1] = backward[...].T
    rate_col[...] = jnp.broadcast_to(rate[...], (128, width)).T
    own = pl.ds(pl.multiple_of(row * count, 16), count)
    both_w = jnp.concatenate([chan[0, own, :], chan[1, own, :]], 0).astype(bf16)
    rates = rate_col[own, 0:1]
    chunk = 512
    energy_ref[...] = jnp.zeros_like(energy_ref)

    def hidden_chunk(i):
        at = pl.ds(i * chunk, chunk)
        hidden = sine_of_turns(dot(feats[at, :], first_w))
        for level in range(INNER):
            h_high, h_low = split_two(hidden)
            wide = dot(jnp.concatenate([h_high, h_low], 1), inner_w[level])
            hidden = sine_of_turns(wide[:, :128] + wide[:, 128:] + inner_p[level : level + 1, :])
        hid[col, at, :] = hidden.astype(bf16)

    def filter_chunk(owner, i):
        at = pl.ds(pl.multiple_of(owner * quarter + i * chunk, chunk), chunk)
        both = lax.dot_general(both_w, hid[owner, pl.ds(i * chunk, chunk), :], (((1,), (1,)), ((), ())),
                               preferred_element_type=f32)
        place = lax.broadcasted_iota(jnp.int32, (count, chunk), 1) + (owner * quarter + i * chunk)
        window = jnp.exp(place.astype(f32) * (-1.0 / (length - 1)) * rates)
        ahead = both[:count] * window
        behind = jnp.where(place == 0, 0.0, both[count:] * window)
        sums[:, at] = ahead + behind
        diffs[:, at] = ahead - behind
        energy_ref[...] += jnp.broadcast_to(
            jnp.sum(ahead * ahead + behind * behind, axis=1, keepdims=True), (count, 128))

    pieces = quarter // chunk
    partner = col + 1 - 2 * lax.rem(col, 2)
    across = lax.rem(col + 2, n_col)

    def pass_on(kind, owner, i, target):
        part = hid.at[owner, pl.ds(i * chunk, chunk)]
        return pltpu.make_async_remote_copy(
            src_ref=part, dst_ref=part, send_sem=hid_s.at[kind, i], recv_sem=hid_r.at[kind, i],
            device_id=(row, target), device_id_type=mesh_id)

    loads[0].wait()
    for i in range(pieces):
        hidden_chunk(i)

    pl.semaphore_wait(barrier, n_row + n_col - 2)
    edges = [
        pltpu.make_async_remote_copy(
            src_ref=tokens_h.at[pl.ds(rows - 16 if i == 0 else 0, 16)],
            dst_ref=tok.at[pl.ds(rows + 16 * i, 16)],
            send_sem=edge_send.at[i], recv_sem=edge_recv.at[i],
            device_id=(lax.rem(row + (1 if i == 0 else n_row - 1), n_row), col), device_id_type=mesh_id)
        for i in range(2)
    ]
    for edge in edges:
        edge.start()
    to_across = [pass_on(0, col, i, across) for i in range(pieces)]
    to_partner = [pass_on(1, col, i, partner) for i in range(pieces)]
    relayed = [pass_on(2, across, i, partner) for i in range(pieces)]
    for copy in to_across + to_partner:
        copy.start()
    loads[1].wait()
    loads[2].wait()
    loads[3].wait()
    for edge in edges:
        edge.wait()

    index = lax.broadcasted_iota(jnp.int32, (rows, width), 0)
    has_before = jnp.where(row > 0, 1.0, 0.0)
    has_after = jnp.where(row < n_row - 1, 1.0, 0.0)

    def convolved(j):
        proj = dot(tok[...], weights[j]).astype(bf16).astype(f32)
        main = proj[:rows]
        first = proj[rows + 15 : rows + 16] * has_before
        last = proj[rows + 16 : rows + 17] * has_after
        before = jnp.where(index == 0, first, pltpu.roll(main, 1, 0))
        after = jnp.where(index == rows - 1, last, pltpu.roll(main, rows - 1, 0))
        return before * taps[0, j : j + 1, :] + main * taps[1, j : j + 1, :] + after * taps[2, j : j + 1, :]

    signal = (convolved(1) * convolved(2)).astype(bf16)
    signal_ref[...] = signal
    flipped = signal.astype(f32).T.astype(bf16)
    for g in range(n_row):
        sig_send[g] = flipped[g * count : (g + 1) * count]

    def exchange(send, recv, s_sem, r_sem, size, me, target):
        copies = []
        for o in range(1, size):
            peer = lax.rem(me + o, size)
            copies.append(pltpu.make_async_remote_copy(
                src_ref=send.at[peer], dst_ref=recv.at[me],
                send_sem=s_sem.at[o], recv_sem=r_sem.at[o], device_id=target(peer), device_id_type=mesh_id))
        for copy in copies:
            copy.start()
        recv[me] = send[me]
        return copies

    along_row = lambda peer: (peer, col)
    along_col = lambda peer: (row, peer)
    travelling = exchange(sig_send, sig_recv, sig_s, sig_r, n_row, row, along_row)

    loads[4].wait()
    gate_ref[...] = convolved(0).astype(bf16)
    for i in range(pieces):
        filter_chunk(col, i)
    for i in range(pieces):
        to_partner[i].wait()
        filter_chunk(partner, i)
    for i in range(pieces):
        to_across[i].wait()
        relayed[i].start()
    for i in range(pieces):
        filter_chunk(across, i)
    for i in range(pieces):
        relayed[i].wait()
        filter_chunk(lax.rem(partner + 2, n_col), i)
    scale_ref[...] = lax.rsqrt(1.0 + energy_ref[...]) * (0.5 / length)

    def turn_into(first, pairs, top, left, weighted):
        for k, (real, imag) in enumerate(pairs):
            c, s = twist_c[k : k + 1, pl.ds(left, 128)], twist_s[k : k + 1, pl.ds(left, 128)]
            if weighted and k not in (0, planes):
                c, s = c * 2.0, s * 2.0
            at = pl.ds(pl.multiple_of(k * count + top, 16), 16)
            if imag is None:
                new_real, new_imag = real * c, -(real * s)
            else:
                new_real, new_imag = real * c + imag * s, imag * c - real * s
            turned[first, at, pl.ds(left, 128)] = new_real.astype(bf16)
            turned[first + 1, at, pl.ds(left, 128)] = new_imag.astype(bf16)

    def filter_tile(top, left):
        scale = scale_ref[pl.ds(top, 16), :]
        for which, source in enumerate((sums, diffs)):
            got = [source[pl.ds(top, 16), pl.ds(pl.multiple_of(r * WIDE + left, 128), 128)] * scale for r in range(planes)]
            turn_into(2 * which, first_stage(got), top, left, True)

    tiles(count, filter_tile)
    filt[0] = dot(turned[0], cos_t[...]) + dot(turned[1], sin_t[...])
    filt[1] = dot(turned[3], cos_t[...]) - dot(turned[2], sin_t[...])
    for copy in travelling:
        copy.wait()

    def signal_tile(top, left):
        got = [sig_recv[r // per, pl.ds(top, 16), pl.ds(pl.multiple_of(r % per * WIDE + left, 128), 128)].astype(f32)
               for r in range(planes)]
        turn_into(0, first_stage(got), top, left, False)

    tiles(count, signal_tile)
    real = dot(turned[0], cos_t[...]) + dot(turned[1], sin_t[...])
    imag = dot(turned[1], cos_t[...]) - dot(turned[0], sin_t[...])
    prod_real = (real * filt[0] - imag * filt[1]).astype(bf16)
    prod_imag = (real * filt[1] + imag * filt[0]).astype(bf16)
    back[0] = dot(prod_real, cos_t[...]) - dot(prod_imag, sin_t[...])
    back[1] = dot(prod_imag, cos_t[...]) + dot(prod_real, sin_t[...])

    def back_tile(top, left):
        pairs = []
        for k in range(planes + 1):
            c, s = twist_c[k : k + 1, pl.ds(left, 128)], twist_s[k : k + 1, pl.ds(left, 128)]
            at = pl.ds(pl.multiple_of(k * count + top, 16), 16)
            b_real, b_imag = back[0, at, pl.ds(left, 128)], back[1, at, pl.ds(left, 128)]
            pairs.append((b_real * c - b_imag * s, b_imag * c + b_real * s))
        for r, plane in enumerate(last_stage(pairs)):
            at = pl.multiple_of(r % per * WIDE + left, 128)
            resp_send[r // per, pl.ds(top, 16), pl.ds(at, 128)] = plane.astype(bf16)

    tiles(count, back_tile)
    for copy in exchange(resp_send, resp_recv, resp_s, resp_r, n_row, row, along_row):
        copy.wait()
    response = jnp.concatenate([resp_recv[g].astype(f32) for g in range(n_row)], 0).T
    mixed = (gate_ref[...].astype(f32) * (response + skip[...] * signal_ref[...].astype(f32))).astype(bf16)
    share = rows // n_col
    for p in range(n_col):
        mix_send[p] = mixed[p * share : (p + 1) * share]
    travelling = exchange(mix_send, mix_recv, mix_s, mix_r, n_col, col, along_col)
    for copy in travelling:
        copy.wait()
    for p in range(n_col):
        out_ref[:, p * width : (p + 1) * width] = mix_recv[p]


def fits(tokens_rows, seq_length, own_width, row_devices, col_devices, units):
    planes = seq_length // WIDE
    members = own_width // row_devices
    return (
        own_width % 128 == 0
        and members % 16 == 0
        and tokens_rows % WIDE == 0
        and seq_length % 512 == 0
        and planes % 8 == 0
        and 8 <= planes <= 32
        and units == 128
        and tokens_rows % 64 == 0
        and col_devices == 4
        and seq_length % 2048 == 0
    )


def on_device_fast(
    tokens, outer_weight, inner_weight, value_weight, conv_taps, feature_weight, feature_phase,
    inner_mats, inner_phase, frequency, forward_weight, backward_weight, decay_rate, skip_gain, output_weight,
):
    f32, bf16 = jnp.float32, jnp.bfloat16
    rows, depth = tokens.shape
    devices = lax.axis_size("row")
    seq_length = rows * devices
    width = outer_weight.shape[1]
    members = width // devices
    planes = seq_length // WIDE
    n_col = lax.axis_size("col")
    k_index = np.arange(planes + 1)[:, None] * np.arange(WIDE)[None, :]
    twist_c = jnp.asarray(np.cos(2 * np.pi * k_index / (2 * seq_length)), f32)
    twist_s = jnp.asarray(np.sin(2 * np.pi * k_index / (2 * seq_length)), f32)
    w_index = np.arange(WIDE)[:, None] * np.arange(WIDE)[None, :] % WIDE
    cos_t = jnp.asarray(np.cos(2 * np.pi * w_index / WIDE), bf16)
    sin_t = jnp.asarray(np.sin(2 * np.pi * w_index / WIDE), bf16)
    spec_rows = (planes + 1) * members
    any_spec = pl.BlockSpec(memory_space=pl.ANY)
    vmem = pl.BlockSpec(memory_space=pltpu.VMEM)
    dma = pltpu.SemaphoreType.DMA
    share = rows // n_col
    pieces = seq_length // n_col // 512
    exchanged = pltpu.VMEM((devices, members, rows), bf16)
    spread = pltpu.VMEM((n_col, share, width), bf16)
    mixed = pl.pallas_call(
        layer_kernel,
        out_shape=jax.ShapeDtypeStruct((share, n_col * width), bf16),
        in_specs=[any_spec] * 5 + [vmem] * 14,
        out_specs=vmem,
        scratch_shapes=[
            pltpu.VMEM((rows + 32, depth), bf16),
            pltpu.VMEM((3, depth, width), bf16),
            pltpu.VMEM((seq_length // n_col, 128), bf16),
            pltpu.VMEM((n_col, seq_length // n_col, 128), bf16),
            exchanged, exchanged, exchanged, exchanged, spread, spread,
            pltpu.VMEM((members, seq_length), f32),
            pltpu.VMEM((members, seq_length), f32),
            pltpu.VMEM((4, spec_rows, WIDE), bf16),
            pltpu.VMEM((2, spec_rows, WIDE), f32),
            pltpu.VMEM((2, spec_rows, WIDE), f32),
            pltpu.VMEM((members, 128), f32),
            pltpu.VMEM((128, 128), f32),
            pltpu.VMEM((2, width, 128), f32),
            pltpu.VMEM((width, 128), f32),
            pltpu.VMEM((members, 128), f32),
            pltpu.VMEM((rows, width), bf16),
            pltpu.VMEM((rows, width), bf16),
            dma((5,)), dma((2,)), dma((2,)), dma((3, pieces)), dma((3, pieces)),
            dma((devices,)), dma((devices,)), dma((devices,)), dma((devices,)), dma((n_col,)), dma((n_col,)),
        ],
        compiler_params=pltpu.CompilerParams(
            collective_id=0, has_side_effects=True, vmem_limit_bytes=GRANT),
        name="layer",
    )(
        tokens, outer_weight, inner_weight, value_weight, jnp.asarray(feature_table(seq_length)),
        conv_taps, feature_weight, feature_phase[None], inner_mats, inner_phase, frequency[None],
        forward_weight, backward_weight, decay_rate[None], skip_gain[None], twist_c, twist_s, cos_t, sin_t,
    )
    return jnp.dot(mixed, output_weight, preferred_element_type=f32).astype(bf16)


GRANT = 54 * 1024 * 1024


def on_any(*args):
    tokens, outer_weight, feature_weight = args[0], args[1], args[5]
    devices = lax.axis_size("row")
    if fits(tokens.shape[0], tokens.shape[0] * devices, outer_weight.shape[1], devices, lax.axis_size("col"), feature_weight.shape[1]):
        return on_device_fast(*args)
    return on_device(*args)


def solution(mesh):
    placed = (
        P("row", None),
        P(None, "col"),
        P(None, "col"),
        P(None, "col"),
        P(None, None, "col"),
        P(),
        P(),
        P(),
        P(),
        P(),
        P(None, "col"),
        P(None, "col"),
        P("col"),
        P("col"),
        P(),
    )
    return jax.shard_map(
        on_any, mesh=mesh, in_specs=placed, out_specs=P(("row", "col"), None), check_vma=False
    )
```

```python
import functools
import math

import jax
import jax.numpy as jnp
import numpy as np
from jax import lax
from jax.experimental import pallas as pl
from jax.experimental.pallas import tpu as pltpu
from jax.sharding import PartitionSpec as P

BANDS = 16
INNER = 2
FACTOR = 256


PRECISE = lax.Precision.HIGHEST


def with_halo(array, sides, width):
    for axis, dim in sides:
        devices, length = (lax.axis_size(axis), array.shape[dim])
        up = [(i, (i + 1) % devices) for i in range(devices - 1)]
        down = [(j, i) for i, j in up]
        last = lax.slice_in_dim(array, length - width, length, axis=dim)
        leading = lax.slice_in_dim(array, 0, width, axis=dim)
        before = lax.ppermute(last, axis, up)
        after = lax.ppermute(leading, axis, down)
        array = jnp.concatenate([before, array, after], axis=dim)
    return array


def phases(height, breadth, period):
    row_index = lax.broadcasted_iota(jnp.int32, (height, breadth), 0)
    col_index = lax.broadcasted_iota(jnp.int32, (height, breadth), 1)
    phase_angle = 2.0 * math.pi / period * (row_index * col_index % period).astype(jnp.float32)
    return (jnp.cos(phase_angle), jnp.sin(phase_angle))


def along_last(operand, matrix):
    return jnp.einsum("ckb,bj->ckj", operand, matrix, precision=PRECISE)


def forward_transform(operand, tables):
    cosine_one, sine_one, twist_cos, twist_sin, cosine_two, sine_two = tables
    used_rows = operand.shape[1]
    first_real = jnp.einsum("kr,crb->ckb", cosine_one[:, :used_rows], operand, precision=PRECISE)
    first_imag = -jnp.einsum("kr,crb->ckb", sine_one[:, :used_rows], operand, precision=PRECISE)
    turned_real = first_real * twist_cos + first_imag * twist_sin
    turned_imag = first_imag * twist_cos - first_real * twist_sin
    spec_real = along_last(turned_real, cosine_two) + along_last(turned_imag, sine_two)
    spec_imag = along_last(turned_imag, cosine_two) - along_last(turned_real, sine_two)
    return (spec_real, spec_imag)


def inverse_transform(spec_real, spec_imag, tables, kept_rows):
    cosine_one, sine_one, twist_cos, twist_sin, cosine_two, sine_two = tables
    back_real = along_last(spec_real, cosine_two) - along_last(spec_imag, sine_two)
    back_imag = along_last(spec_imag, cosine_two) + along_last(spec_real, sine_two)
    untwist_real = back_real * twist_cos - back_imag * twist_sin
    untwist_imag = back_imag * twist_cos + back_real * twist_sin
    return jnp.einsum(
        "nk,ckb->cnb", cosine_one[:kept_rows], untwist_real, precision=PRECISE
    ) - jnp.einsum("nk,ckb->cnb", sine_one[:kept_rows], untwist_imag, precision=PRECISE)


def position_filters(
    places,
    seq_length,
    feature_weight,
    feature_phase,
    inner_mats,
    inner_phase,
    frequency,
    forward_cols,
    backward_cols,
    rates,
):
    scaled = places.astype(jnp.float32) / (seq_length - 1)
    band_ints = 1 + jnp.arange(BANDS, dtype=jnp.int32) * (seq_length // (4 * BANDS))
    turns = places[:, None] * band_ints[None, :] % seq_length
    angles = 2.0 * math.pi / seq_length * turns.astype(jnp.float32)
    features = jnp.concatenate([scaled[:, None], jnp.cos(angles), -jnp.sin(angles)], axis=1)
    hidden = jnp.sin(
        frequency * (jnp.dot(features, feature_weight, precision=PRECISE) + feature_phase)
    )
    for level_index in range(INNER):
        hidden = jnp.sin(
            frequency
            * (
                jnp.dot(hidden, inner_mats[level_index], precision=PRECISE)
                + inner_phase[level_index]
            )
        )
    window = jnp.exp(-scaled[:, None] * rates[None, :])
    filter_ahead = jnp.dot(hidden, forward_cols, precision=PRECISE) * window
    filter_behind = jnp.dot(hidden, backward_cols, precision=PRECISE) * window
    return (filter_ahead, filter_behind)


def on_device(
    tokens,
    outer_weight,
    inner_weight,
    value_weight,
    conv_taps,
    feature_weight,
    feature_phase,
    inner_mats,
    inner_phase,
    frequency,
    forward_weight,
    backward_weight,
    decay_rate,
    skip_gain,
    output_weight,
):
    block_rows = tokens.shape[0]
    seq_length = block_rows * lax.axis_size("row")
    own_width = outer_weight.shape[1]
    outer_proj = jnp.dot(tokens, outer_weight, preferred_element_type=jnp.float32).astype(
        jnp.bfloat16
    )
    inner_proj = jnp.dot(tokens, inner_weight, preferred_element_type=jnp.float32).astype(
        jnp.bfloat16
    )
    value_proj = jnp.dot(tokens, value_weight, preferred_element_type=jnp.float32).astype(
        jnp.bfloat16
    )
    stacked = jnp.concatenate([outer_proj, inner_proj, value_proj], axis=1)
    padded = with_halo(stacked, (("row", 0),), 1).astype(jnp.float32)
    tap_table = conv_taps.reshape(3, 3 * own_width)
    convolved = padded[:-2] * tap_table[0] + padded[1:-1] * tap_table[1] + padded[2:] * tap_table[2]
    gate_part = convolved[:, :own_width].astype(jnp.bfloat16)
    signal = (convolved[:, own_width : 2 * own_width] * convolved[:, 2 * own_width :]).astype(
        jnp.bfloat16
    )
    offset = lax.axis_index("row") * block_rows
    places = offset + jnp.arange(block_rows, dtype=jnp.int32)
    filter_ahead, filter_behind = position_filters(
        places,
        seq_length,
        feature_weight,
        feature_phase,
        inner_mats,
        inner_phase,
        frequency,
        forward_weight,
        backward_weight,
        decay_rate,
    )
    moved_signal, moved_ahead, moved_behind = (
        lax.all_to_all(signal.astype(jnp.float32), "row", split_axis=1, concat_axis=0, tiled=True),
        lax.all_to_all(filter_ahead, "row", split_axis=1, concat_axis=0, tiled=True),
        lax.all_to_all(filter_behind, "row", split_axis=1, concat_axis=0, tiled=True),
    )
    per_device = moved_ahead.shape[1]
    ahead_rows = moved_ahead.T
    behind_rows = moved_behind.T
    norm_scale = lax.rsqrt(
        1.0
        + jnp.sum(jnp.square(ahead_rows), axis=1)
        + jnp.sum(jnp.square(behind_rows[:, 1:]), axis=1)
    )
    kernel_rows = (
        jnp.concatenate(
            [ahead_rows, jnp.zeros((per_device, 1), jnp.float32), jnp.flip(behind_rows[:, 1:], 1)],
            axis=1,
        )
        * norm_scale[:, None]
    )
    padded_length = 2 * seq_length
    height = padded_length // FACTOR
    tables = (
        phases(height, height, height)
        + phases(height, FACTOR, padded_length)
        + phases(FACTOR, FACTOR, FACTOR)
    )
    kernel_real, kernel_imag = forward_transform(
        kernel_rows.reshape(per_device, height, FACTOR), tables
    )
    signal_real, signal_imag = forward_transform(
        moved_signal.T.reshape(per_device, height // 2, FACTOR), tables
    )
    prod_real = signal_real * kernel_real - signal_imag * kernel_imag
    prod_imag = signal_real * kernel_imag + signal_imag * kernel_real
    response = inverse_transform(prod_real, prod_imag, tables, height // 2) / padded_length
    response = response.reshape(per_device, seq_length).T.astype(jnp.bfloat16)
    returned = lax.all_to_all(response, "row", split_axis=0, concat_axis=1, tiled=True)
    mixed_rows = (
        gate_part.astype(jnp.float32)
        * (returned.astype(jnp.float32) + skip_gain * signal.astype(jnp.float32))
    ).astype(jnp.bfloat16)
    whole_rows = lax.all_to_all(mixed_rows, "col", split_axis=0, concat_axis=1, tiled=True)
    return jnp.dot(whole_rows, output_weight, preferred_element_type=jnp.float32).astype(
        jnp.bfloat16
    )


WIDE = 256


def feature_table(seq_length):
    places = np.arange(seq_length, dtype=np.int64)
    bands = 1 + np.arange(BANDS, dtype=np.int64) * (seq_length // (4 * BANDS))
    angles = 2.0 * np.pi / seq_length * (places[:, None] * bands[None, :] % seq_length)
    scaled = places / (seq_length - 1)
    feats = np.concatenate([scaled[:, None], np.cos(angles), -np.sin(angles)], 1).astype(np.float32)
    high = feats.astype(jnp.bfloat16)
    low = (feats - high.astype(np.float32)).astype(jnp.bfloat16)
    used = np.zeros((seq_length, 128), jnp.bfloat16)
    count = feats.shape[1]
    for start, part in ((0, high), (40, low), (80, high)):
        used[:, start : start + count] = part
    used[:, 120:122] = 1
    return used


def sine_coefficients():
    u = 0.5 * np.cos(np.pi * (np.arange(4000) + 0.5) / 8000)
    powers = np.stack([u ** (2 * i + 1) for i in range(6)], 1)
    return [float(v) for v in np.linalg.lstsq(powers, np.sin(2 * np.pi * u), rcond=None)[0]]


SINE = sine_coefficients()
MAGIC = 12582912.0


def sine_of_turns(turns):
    u = turns - ((turns + MAGIC) - MAGIC)
    square = u * u
    total = SINE[-1]
    for value in SINE[-2::-1]:
        total = total * square + value
    return u * total


def split_two(value):
    high = value.astype(jnp.bfloat16)
    return high, (value - high.astype(jnp.float32)).astype(jnp.bfloat16)


def combine(terms):
    total = None
    for coef, array in terms:
        if abs(coef) < 1e-9:
            continue
        if abs(abs(coef) - 1.0) < 1e-9:
            if total is None:
                total = array if coef > 0 else -array
            else:
                total = total + array if coef > 0 else total - array
        else:
            total = array * coef if total is None else total + array * coef
    return total


def first_stage(planes):
    half = len(planes)
    full, mid = 2 * half, half // 2
    quarter = mid // 2
    theta = 2 * math.pi / full
    add = {r: planes[r] + planes[half - r] for r in range(1, mid)}
    sub = {r: planes[r] - planes[half - r] for r in range(1, mid)}
    add_add = {r: add[r] + add[mid - r] for r in range(1, quarter)}
    add_sub = {r: add[r] - add[mid - r] for r in range(1, quarter)}
    sub_add = {r: sub[r] + sub[mid - r] for r in range(1, quarter)}
    sub_sub = {r: sub[r] - sub[mid - r] for r in range(1, quarter)}
    ends = (planes[0] + planes[mid], planes[0] - planes[mid])
    out = []
    for k in range(half + 1):
        cos = lambda r: math.cos(theta * r * k)
        sin = lambda r: math.sin(theta * r * k)
        if k % 4 == 0:
            real = combine([(1.0, ends[0]), (cos(quarter), add[quarter])] + [(cos(r), add_add[r]) for r in add_add])
            imag = combine([(-sin(r), sub_sub[r]) for r in sub_sub])
        elif k % 2 == 0:
            real = combine([(1.0, ends[1])] + [(cos(r), add_sub[r]) for r in add_sub])
            imag = combine([(-sin(quarter), sub[quarter])] + [(-sin(r), sub_add[r]) for r in sub_add])
        else:
            real = combine([(1.0, planes[0])] + [(cos(r), sub[r]) for r in sub])
            imag = combine([(-sin(mid), planes[mid])] + [(-sin(r), add[r]) for r in add])
        out.append((real, imag))
    return out


def last_stage(pairs):
    half = len(pairs) - 1
    full, mid = 2 * half, half // 2
    quarter = mid // 2
    theta = 2 * math.pi / full
    four = range(0, half + 1, 4)
    two = range(2, half + 1, 4)
    odd = range(1, half + 1, 2)
    real = [p[0] for p in pairs]
    imag = [p[1] for p in pairs]
    out = [None] * half

    def cosines(r, ks):
        return combine([(math.cos(theta * r * k), real[k]) for k in ks])

    def sines(r, ks):
        return combine([(math.sin(theta * r * k), imag[k]) for k in ks])

    out[0] = combine([(1.0, v) for v in real])
    out[mid] = cosines(mid, list(four) + list(two)) - sines(mid, odd)

    def place(r, cos_even, sin_even):
        cos_odd, sin_odd = cosines(r, odd), sines(r, odd)
        out[r] = (cos_even - sin_even) + (cos_odd - sin_odd)
        out[half - r] = (cos_even + sin_even) - (cos_odd + sin_odd)

    for r in range(1, quarter):
        c0, c2, s0, s2 = cosines(r, four), cosines(r, two), sines(r, four), sines(r, two)
        place(r, c0 + c2, s0 + s2)
        place(mid - r, c0 - c2, s2 - s0)
    place(quarter, cosines(quarter, four), sines(quarter, two))
    return out


def tiles(count, body):
    lanes = WIDE // 128

    def one(i, carry):
        body(pl.multiple_of(i // lanes * 16, 16), pl.multiple_of(i % lanes * 128, 128))
        return carry

    lax.fori_loop(0, count // 16 * lanes, one, 0)


def layer_kernel(
    tokens_h, outer_h, inner_h, value_h, feats_h,
    taps, feature_weight, feature_phase, inner_mats, inner_phase, frequency, forward, backward, rate, skip,
    twist_c, twist_s, cos_t, sin_t,
    out_ref,
    tok, weights, feats, hid, sig_send, sig_recv, resp_send, resp_recv, mix_send, mix_recv,
    sums, diffs, turned, filt, back, scale_ref, first_ref, chan, rate_col, energy_ref, gate_ref, signal_ref,
    local_sem, edge_send, edge_recv, hid_s, hid_r, sig_s, sig_r, resp_s, resp_r, mix_s, mix_r,
):
    f32, bf16 = jnp.float32, jnp.bfloat16
    dot = functools.partial(jnp.dot, preferred_element_type=f32)
    n_row, n_col = lax.axis_size("row"), lax.axis_size("col")
    row, col = lax.axis_index("row"), lax.axis_index("col")
    length, rows = feats_h.shape[0], tokens_h.shape[0]
    quarter = length // n_col
    width = outer_h.shape[1]
    count = width // n_row
    planes = length // WIDE
    per = rows // WIDE
    mesh_id = pl.DeviceIdType.MESH

    barrier = pltpu.get_barrier_semaphore()
    for o in range(1, n_row):
        pl.semaphore_signal(barrier, inc=1, device_id=(lax.rem(row + o, n_row), col), device_id_type=mesh_id)
    for o in range(1, n_col):
        pl.semaphore_signal(barrier, inc=1, device_id=(row, lax.rem(col + o, n_col)), device_id_type=mesh_id)
    loads = [
        pltpu.make_async_copy(
            feats_h.at[pl.ds(pl.multiple_of(col * quarter, 512), quarter)], feats, local_sem.at[0]),
        pltpu.make_async_copy(tokens_h, tok.at[pl.ds(0, rows)], local_sem.at[1]),
        pltpu.make_async_copy(inner_h, weights.at[1], local_sem.at[2]),
        pltpu.make_async_copy(value_h, weights.at[2], local_sem.at[3]),
        pltpu.make_async_copy(outer_h, weights.at[0], local_sem.at[4]),
    ]
    for load in loads:
        load.start()

    turn = frequency[...] * (0.5 / math.pi)
    high, low = split_two(feature_weight[...] * turn)
    phase_high, phase_low = split_two(feature_phase[...] * turn)
    used = high.shape[0]
    first_ref[...] = jnp.zeros_like(first_ref)
    first_ref[0:used] = high.astype(f32)
    first_ref[40 : 40 + used] = high.astype(f32)
    first_ref[80 : 80 + used] = low.astype(f32)
    first_ref[120:121] = phase_high.astype(f32)
    first_ref[121:122] = phase_low.astype(f32)
    first_w = first_ref[...].astype(bf16)
    inner_w = []
    for level in range(INNER):
        mat_high, mat_low = split_two(inner_mats[level] * turn)
        inner_w.append(jnp.concatenate([
            jnp.concatenate([mat_high, mat_low], 1), jnp.concatenate([mat_high, jnp.zeros_like(mat_low)], 1)], 0))
    inner_p = inner_phase[...] * turn
    chan[0] = forward[...].T
    chan[1] = backward[...].T
    rate_col[...] = jnp.broadcast_to(rate[...], (128, width)).T
    own = pl.ds(pl.multiple_of(row * count, 16), count)
    both_w = jnp.concatenate([chan[0, own, :], chan[1, own, :]], 0).astype(bf16)
    rates = rate_col[own, 0:1]
    chunk = 512
    energy_ref[...] = jnp.zeros_like(energy_ref)

    def hidden_chunk(i):
        at = pl.ds(i * chunk, chunk)
        hidden = sine_of_turns(dot(feats[at, :], first_w))
        for level in range(INNER):
            h_high, h_low = split_two(hidden)
            wide = dot(jnp.concatenate([h_high, h_low], 1), inner_w[level])
            hidden = sine_of_turns(wide[:, :128] + wide[:, 128:] + inner_p[level : level + 1, :])
        hid[col, at, :] = hidden.astype(bf16)

    def filter_chunk(owner, i):
        at = pl.ds(pl.multiple_of(owner * quarter + i * chunk, chunk), chunk)
        both = lax.dot_general(both_w, hid[owner, pl.ds(i * chunk, chunk), :], (((1,), (1,)), ((), ())),
                               preferred_element_type=f32)
        place = lax.broadcasted_iota(jnp.int32, (count, chunk), 1) + (owner * quarter + i * chunk)
        window = jnp.exp(place.astype(f32) * (-1.0 / (length - 1)) * rates)
        ahead = both[:count] * window
        behind = jnp.where(place == 0, 0.0, both[count:] * window)
        sums[:, at] = ahead + behind
        diffs[:, at] = ahead - behind
        energy_ref[...] += jnp.broadcast_to(
            jnp.sum(ahead * ahead + behind * behind, axis=1, keepdims=True), (count, 128))

    pieces = quarter // chunk
    partner = col + 1 - 2 * lax.rem(col, 2)
    across = lax.rem(col + 2, n_col)

    def pass_on(kind, owner, i, target):
        part = hid.at[owner, pl.ds(i * chunk, chunk)]
        return pltpu.make_async_remote_copy(
            src_ref=part, dst_ref=part, send_sem=hid_s.at[kind, i], recv_sem=hid_r.at[kind, i],
            device_id=(row, target), device_id_type=mesh_id)

    loads[0].wait()
    for i in range(pieces):
        hidden_chunk(i)

    pl.semaphore_wait(barrier, n_row + n_col - 2)
    edges = [
        pltpu.make_async_remote_copy(
            src_ref=tokens_h.at[pl.ds(rows - 16 if i == 0 else 0, 16)],
            dst_ref=tok.at[pl.ds(rows + 16 * i, 16)],
            send_sem=edge_send.at[i], recv_sem=edge_recv.at[i],
            device_id=(lax.rem(row + (1 if i == 0 else n_row - 1), n_row), col), device_id_type=mesh_id)
        for i in range(2)
    ]
    for edge in edges:
        edge.start()
    to_across = [pass_on(0, col, i, across) for i in range(pieces)]
    to_partner = [pass_on(1, col, i, partner) for i in range(pieces)]
    relayed = [pass_on(2, across, i, partner) for i in range(pieces)]
    for copy in to_across + to_partner:
        copy.start()
    loads[1].wait()
    loads[2].wait()
    loads[3].wait()
    for edge in edges:
        edge.wait()

    index = lax.broadcasted_iota(jnp.int32, (rows, width), 0)
    has_before = jnp.where(row > 0, 1.0, 0.0)
    has_after = jnp.where(row < n_row - 1, 1.0, 0.0)

    def convolved(j):
        proj = dot(tok[...], weights[j]).astype(bf16).astype(f32)
        main = proj[:rows]
        first = proj[rows + 15 : rows + 16] * has_before
        last = proj[rows + 16 : rows + 17] * has_after
        before = jnp.where(index == 0, first, pltpu.roll(main, 1, 0))
        after = jnp.where(index == rows - 1, last, pltpu.roll(main, rows - 1, 0))
        return before * taps[0, j : j + 1, :] + main * taps[1, j : j + 1, :] + after * taps[2, j : j + 1, :]

    signal = (convolved(1) * convolved(2)).astype(bf16)
    signal_ref[...] = signal
    flipped = signal.astype(f32).T.astype(bf16)
    for g in range(n_row):
        sig_send[g] = flipped[g * count : (g + 1) * count]

    def exchange(send, recv, s_sem, r_sem, size, me, target):
        copies = []
        for o in range(1, size):
            peer = lax.rem(me + o, size)
            copies.append(pltpu.make_async_remote_copy(
                src_ref=send.at[peer], dst_ref=recv.at[me],
                send_sem=s_sem.at[o], recv_sem=r_sem.at[o], device_id=target(peer), device_id_type=mesh_id))
        for copy in copies:
            copy.start()
        recv[me] = send[me]
        return copies

    along_row = lambda peer: (peer, col)
    along_col = lambda peer: (row, peer)
    travelling = exchange(sig_send, sig_recv, sig_s, sig_r, n_row, row, along_row)

    loads[4].wait()
    gate_ref[...] = convolved(0).astype(bf16)
    for i in range(pieces):
        filter_chunk(col, i)
    for i in range(pieces):
        to_partner[i].wait()
        filter_chunk(partner, i)
    for i in range(pieces):
        to_across[i].wait()
        relayed[i].start()
    for i in range(pieces):
        filter_chunk(across, i)
    for i in range(pieces):
        relayed[i].wait()
        filter_chunk(lax.rem(partner + 2, n_col), i)
    scale_ref[...] = lax.rsqrt(1.0 + energy_ref[...]) * (0.5 / length)

    def turn_into(first, pairs, top, left, weighted):
        for k, (real, imag) in enumerate(pairs):
            c, s = twist_c[k : k + 1, pl.ds(left, 128)], twist_s[k : k + 1, pl.ds(left, 128)]
            if weighted and k not in (0, planes):
                c, s = c * 2.0, s * 2.0
            at = pl.ds(pl.multiple_of(k * count + top, 16), 16)
            if imag is None:
                new_real, new_imag = real * c, -(real * s)
            else:
                new_real, new_imag = real * c + imag * s, imag * c - real * s
            turned[first, at, pl.ds(left, 128)] = new_real.astype(bf16)
            turned[first + 1, at, pl.ds(left, 128)] = new_imag.astype(bf16)

    def filter_tile(top, left):
        scale = scale_ref[pl.ds(top, 16), :]
        for which, source in enumerate((sums, diffs)):
            got = [source[pl.ds(top, 16), pl.ds(pl.multiple_of(r * WIDE + left, 128), 128)] * scale for r in range(planes)]
            turn_into(2 * which, first_stage(got), top, left, True)

    tiles(count, filter_tile)
    filt[0] = dot(turned[0], cos_t[...]) + dot(turned[1], sin_t[...])
    filt[1] = dot(turned[3], cos_t[...]) - dot(turned[2], sin_t[...])
    for copy in travelling:
        copy.wait()

    def signal_tile(top, left):
        got = [sig_recv[r // per, pl.ds(top, 16), pl.ds(pl.multiple_of(r % per * WIDE + left, 128), 128)].astype(f32)
               for r in range(planes)]
        turn_into(0, first_stage(got), top, left, False)

    tiles(count, signal_tile)
    real = dot(turned[0], cos_t[...]) + dot(turned[1], sin_t[...])
    imag = dot(turned[1], cos_t[...]) - dot(turned[0], sin_t[...])
    prod_real = (real * filt[0] - imag * filt[1]).astype(bf16)
    prod_imag = (real * filt[1] + imag * filt[0]).astype(bf16)
    back[0] = dot(prod_real, cos_t[...]) - dot(prod_imag, sin_t[...])
    back[1] = dot(prod_imag, cos_t[...]) + dot(prod_real, sin_t[...])

    def back_tile(top, left):
        pairs = []
        for k in range(planes + 1):
            c, s = twist_c[k : k + 1, pl.ds(left, 128)], twist_s[k : k + 1, pl.ds(left, 128)]
            at = pl.ds(pl.multiple_of(k * count + top, 16), 16)
            b_real, b_imag = back[0, at, pl.ds(left, 128)], back[1, at, pl.ds(left, 128)]
            pairs.append((b_real * c - b_imag * s, b_imag * c + b_real * s))
        for r, plane in enumerate(last_stage(pairs)):
            at = pl.multiple_of(r % per * WIDE + left, 128)
            resp_send[r // per, pl.ds(top, 16), pl.ds(at, 128)] = plane.astype(bf16)

    def back_step(top, i, carry):
        back_tile(top, pl.multiple_of(i * 128, 128))
        return carry

    travelling = []
    for h in range(count // 16):
        lax.fori_loop(0, WIDE // 128, functools.partial(back_step, h * 16), 0)
        for o in range(1, n_row):
            peer = lax.rem(row + o, n_row)
            travelling.append(pltpu.make_async_remote_copy(
                src_ref=resp_send.at[peer, pl.ds(h * 16, 16)], dst_ref=resp_recv.at[row, pl.ds(h * 16, 16)],
                send_sem=resp_s.at[h, o], recv_sem=resp_r.at[h, o],
                device_id=along_row(peer), device_id_type=mesh_id))
            travelling[-1].start()
    resp_recv[row] = resp_send[row]
    for copy in travelling:
        copy.wait()
    response = jnp.concatenate([resp_recv[g].astype(f32) for g in range(n_row)], 0).T
    mixed = (gate_ref[...].astype(f32) * (response + skip[...] * signal_ref[...].astype(f32))).astype(bf16)
    share = rows // n_col
    for p in range(n_col):
        mix_send[p] = mixed[p * share : (p + 1) * share]
    travelling = exchange(mix_send, mix_recv, mix_s, mix_r, n_col, col, along_col)
    for copy in travelling:
        copy.wait()
    for p in range(n_col):
        out_ref[:, p * width : (p + 1) * width] = mix_recv[p]


def fits(tokens_rows, seq_length, own_width, row_devices, col_devices, units):
    planes = seq_length // WIDE
    members = own_width // row_devices
    return (
        own_width % 128 == 0
        and members % 16 == 0
        and tokens_rows % WIDE == 0
        and seq_length % 512 == 0
        and planes % 8 == 0
        and 8 <= planes <= 32
        and units == 128
        and tokens_rows % 64 == 0
        and col_devices == 4
        and seq_length % 2048 == 0
    )


def on_device_fast(
    tokens, outer_weight, inner_weight, value_weight, conv_taps, feature_weight, feature_phase,
    inner_mats, inner_phase, frequency, forward_weight, backward_weight, decay_rate, skip_gain, output_weight,
):
    f32, bf16 = jnp.float32, jnp.bfloat16
    rows, depth = tokens.shape
    devices = lax.axis_size("row")
    seq_length = rows * devices
    width = outer_weight.shape[1]
    members = width // devices
    planes = seq_length // WIDE
    n_col = lax.axis_size("col")
    k_index = np.arange(planes + 1)[:, None] * np.arange(WIDE)[None, :]
    twist_c = jnp.asarray(np.cos(2 * np.pi * k_index / (2 * seq_length)), f32)
    twist_s = jnp.asarray(np.sin(2 * np.pi * k_index / (2 * seq_length)), f32)
    w_index = np.arange(WIDE)[:, None] * np.arange(WIDE)[None, :] % WIDE
    cos_t = jnp.asarray(np.cos(2 * np.pi * w_index / WIDE), bf16)
    sin_t = jnp.asarray(np.sin(2 * np.pi * w_index / WIDE), bf16)
    spec_rows = (planes + 1) * members
    any_spec = pl.BlockSpec(memory_space=pl.ANY)
    vmem = pl.BlockSpec(memory_space=pltpu.VMEM)
    dma = pltpu.SemaphoreType.DMA
    share = rows // n_col
    pieces = seq_length // n_col // 512
    exchanged = pltpu.VMEM((devices, members, rows), bf16)
    spread = pltpu.VMEM((n_col, share, width), bf16)
    mixed = pl.pallas_call(
        layer_kernel,
        out_shape=jax.ShapeDtypeStruct((share, n_col * width), bf16),
        in_specs=[any_spec] * 5 + [vmem] * 14,
        out_specs=vmem,
        scratch_shapes=[
            pltpu.VMEM((rows + 32, depth), bf16),
            pltpu.VMEM((3, depth, width), bf16),
            pltpu.VMEM((seq_length // n_col, 128), bf16),
            pltpu.VMEM((n_col, seq_length // n_col, 128), bf16),
            exchanged, exchanged, exchanged, exchanged, spread, spread,
            pltpu.VMEM((members, seq_length), f32),
            pltpu.VMEM((members, seq_length), f32),
            pltpu.VMEM((4, spec_rows, WIDE), bf16),
            pltpu.VMEM((2, spec_rows, WIDE), f32),
            pltpu.VMEM((2, spec_rows, WIDE), f32),
            pltpu.VMEM((members, 128), f32),
            pltpu.VMEM((128, 128), f32),
            pltpu.VMEM((2, width, 128), f32),
            pltpu.VMEM((width, 128), f32),
            pltpu.VMEM((members, 128), f32),
            pltpu.VMEM((rows, width), bf16),
            pltpu.VMEM((rows, width), bf16),
            dma((5,)), dma((2,)), dma((2,)), dma((3, pieces)), dma((3, pieces)),
            dma((devices,)), dma((devices,)), dma((members // 16, devices)), dma((members // 16, devices)), dma((n_col,)), dma((n_col,)),
        ],
        compiler_params=pltpu.CompilerParams(
            collective_id=0, has_side_effects=True, vmem_limit_bytes=GRANT),
        name="layer",
    )(
        tokens, outer_weight, inner_weight, value_weight, jnp.asarray(feature_table(seq_length)),
        conv_taps, feature_weight, feature_phase[None], inner_mats, inner_phase, frequency[None],
        forward_weight, backward_weight, decay_rate[None], skip_gain[None], twist_c, twist_s, cos_t, sin_t,
    )
    return jnp.dot(mixed, output_weight, preferred_element_type=f32).astype(bf16)


GRANT = 54 * 1024 * 1024


def on_any(*args):
    tokens, outer_weight, feature_weight = args[0], args[1], args[5]
    devices = lax.axis_size("row")
    if fits(tokens.shape[0], tokens.shape[0] * devices, outer_weight.shape[1], devices, lax.axis_size("col"), feature_weight.shape[1]):
        return on_device_fast(*args)
    return on_device(*args)


def solution(mesh):
    placed = (
        P("row", None),
        P(None, "col"),
        P(None, "col"),
        P(None, "col"),
        P(None, None, "col"),
        P(),
        P(),
        P(),
        P(),
        P(),
        P(None, "col"),
        P(None, "col"),
        P("col"),
        P("col"),
        P(),
    )
    return jax.shard_map(
        on_any, mesh=mesh, in_specs=placed, out_specs=P(("row", "col"), None), check_vma=False
    )
```
